512 devices in a mesh: grp: 2 (over y), sp: 16 (over z), tp: 16 (over x, core).
Axes of the slice: x: 8, y: 2, z: 16, core: 2. Of those that a mesh axis runs over, the one named last changes fastest.
The devices are a block of a 8x8x16 slice.
Arguments:
- latent: bfloat16 [16384, 4096], P(('grp', 'sp'), 'tp'), parts along dimension 0, may hold values from -42 to 42
- context: bfloat16 [2048, 4096], P(('grp', 'sp'), 'tp'), parts along dimension 0, may hold values from -42 to 42
- conditions: float32 [4, 4096], P('grp', 'sp'), parts along dimension 0, may hold values from -6 to 6
- mod_weight: bfloat16 [4096, 3, 4096], P('sp', None, 'tp'), may hold values from -0.09375 to 0.09375
- norm_gain: float32 [4096], P('tp'), may hold values from 0.1 to 1.9
- w_query: bfloat16 [4096, 2048], P(None, 'tp'), may hold values from -0.09375 to 0.09375
- w_key: bfloat16 [4096, 2048], P(None, 'tp'), may hold values from -0.09375 to 0.09375
- w_value: bfloat16 [4096, 2048], P(None, 'tp'), may hold values from -0.09375 to 0.09375
- query_gain: float32 [64], replicated, may hold values from 1 to 14
- key_gain: float32 [64], replicated, may hold values from 1 to 14
- lambdas: float32 [16], P('tp'), may hold values from 0.3 to 0.8
- out_gain: float32 [128], replicated, may hold values from 0.1 to 1.9
- w_out: bfloat16 [2048, 4096], P(None, 'tp'), may hold values from -0.125 to 0.125
Outputs:
- updated: bfloat16 [16384, 4096], P(('grp', 'sp'), 'tp'), parts along dimension 0
The draws below stay inside these ranges and needn't reach their ends.
There are 2 independent parts, one for each index of `grp`. The reference program is written for one: setup_inputs(seed, part) draws one part's arguments, and reference() takes and returns one part's arrays. A program takes and returns all parts, laid end to end along the dimension named above; an argument that names none is the same for every part. Nothing has to cross between parts.
All inputs are finite; a program needn't handle non-finite values.
Results may differ from the reference program's by a relative error of at most 0.0076.
Values may be sent and summed in bfloat16 or wider, within the bound.
A program may use at most 64 MiB of HBM per device.

```python
import math
import jax
import jax.numpy as jnp
from jax import lax

D = 4096
HEADS = 16
DK = 64
DV = 128
GRID_W = 64
CTX = 1024
LAT = 8192


def rising_rows(key, row_count):
    column = jnp.arange(D, dtype=jnp.float32)
    base = jnp.clip(jax.random.normal(key, (row_count, D), jnp.float32), -6.0, 6.0)
    return base * (1.0 + 2.0 * column / (D - 1))


def spiked_gains(key, which):
    own_key = jax.random.fold_in(key, which)
    return jax.random.uniform(own_key, (DK,), jnp.float32, 1.1, 1.5)


def draw_latent(key, part):
    return rising_rows(jax.random.fold_in(key, 21), LAT).astype(jnp.bfloat16)


def draw_context(key, part):
    return rising_rows(jax.random.fold_in(key, 22), CTX).astype(jnp.bfloat16)


def draw_query_gain(key, part):
    return spiked_gains(key, 1)


def draw_key_gain(key, part):
    return spiked_gains(key, 2)


def shard_levels(key, extent, pieces, smallest, high):
    loudness = 1.0
    for dim, parts in pieces:
        heights = jax.random.uniform(jax.random.fold_in(jax.random.fold_in(key, 6), dim), (parts,), jnp.float32, smallest / len(pieces), high / len(pieces))
        loudness = loudness * jnp.repeat(jnp.exp(heights), extent[dim] // parts).reshape((-1,) + (1,) * (len(extent) - 1 - dim))
    return loudness


def bell_draw(key, dims, deviation, most, shards=(), kind=jnp.bfloat16):
    result = deviation * jax.random.normal(key, dims, jnp.float32)
    if shards:
        result = result * shard_levels(key, dims, shards, -0.22, 0.18)
    return jnp.clip(result, -most, most).astype(kind)


def setup_inputs(seed: int = 0, part: int = 0) -> dict:
    keys = jax.random.split(jax.random.key(seed), 14)
    own_keys = jax.random.split(jax.random.fold_in(keys[13], part), 14)
    latent = draw_latent(jax.random.fold_in(jax.random.fold_in(keys[13], part), 71), part)
    context = draw_context(jax.random.fold_in(jax.random.fold_in(keys[13], part), 71), part)
    conditions = bell_draw(own_keys[2], (2, D), 1.0, 6.0, ((1, 16),), jnp.float32)
    mod_weight = bell_draw(keys[3], (D, 3, D), D ** -0.5, 0.09375, ((0, 16), (2, 16)))
    norm_gain = jnp.clip(1.0 + 0.18 * jax.random.normal(keys[4], (D,), jnp.float32), 0.1, 1.9)
    w_query = bell_draw(keys[5], (D, HEADS * 2 * DK), D ** -0.5, 0.09375, ((1, 16),))
    w_key = bell_draw(keys[6], (D, HEADS * 2 * DK), D ** -0.5, 0.09375, ((1, 16),))
    w_value = bell_draw(keys[7], (D, HEADS * DV), D ** -0.5, 0.09375, ((1, 16),))
    query_gain = draw_query_gain(jax.random.fold_in(keys[13], 71), part)
    key_gain = draw_key_gain(jax.random.fold_in(keys[13], 71), part)
    lambdas = jnp.clip(0.3 + 0.5 * jax.random.uniform(keys[10], (HEADS,), jnp.float32) ** shard_levels(keys[10], (HEADS,), ((0, 16),), -0.2, 0.2), 0.3, 0.8)
    out_gain = jnp.clip(1.0 + 0.18 * jax.random.normal(keys[11], (DV,), jnp.float32), 0.1, 1.9)
    w_out = bell_draw(keys[12], (HEADS * DV, D), (HEADS * DV) ** -0.5, 0.125, ((1, 16),))
    return {"latent": latent, "context": context, "conditions": conditions, "mod_weight": mod_weight, "norm_gain": norm_gain, "w_query": w_query, "w_key": w_key, "w_value": w_value, "query_gain": query_gain, "key_gain": key_gain, "lambdas": lambdas, "out_gain": out_gain, "w_out": w_out}


epsilon = 1e-06

def turn_half(halves, angles):
    quarter = halves.shape[-1] // 2
    cosine = jnp.cos(angles)[:, None, None, :]
    sine_part = jnp.sin(angles)[:, None, None, :]
    first_part = halves[..., :quarter]
    second = halves[..., quarter:]
    return jnp.concatenate([first_part * cosine - second * sine_part, first_part * sine_part + second * cosine], axis=-1)

def rotate(features, positions):
    half_width = features.shape[-1] // 2
    quarter = half_width // 2
    inverse = 10000.0 ** (-2.0 * jnp.arange(quarter, dtype=jnp.float32) / half_width)
    grid_row = (positions // GRID_W).astype(jnp.float32)
    grid_column = (positions % GRID_W).astype(jnp.float32)
    return jnp.concatenate([turn_half(features[..., :half_width], grid_row[:, None] * inverse), turn_half(features[..., half_width:], grid_column[:, None] * inverse)], axis=-1)

def head_norm(features, gain_row):
    return features * lax.rsqrt(lax.optimization_barrier(jnp.mean(features * features, axis=-1, keepdims=True)) + epsilon) * gain_row

def modulate(rows_in, gain_row, shift_row, scale_row):
    floats = rows_in.astype(jnp.float32)
    factor = lax.rsqrt(lax.optimization_barrier(jnp.mean(floats * floats, axis=1, keepdims=True)) + epsilon)
    return (floats * factor * gain_row * (1.0 + scale_row) + shift_row).astype(jnp.bfloat16)

def reference(latent, context, conditions, mod_weight, norm_gain, w_query, w_key, w_value, query_gain, key_gain, lambdas, out_gain, w_out):
    activated = jax.nn.silu(conditions).astype(jnp.bfloat16)
    modulation = jnp.dot(activated, mod_weight.reshape(D, 3 * D), preferred_element_type=jnp.float32).reshape(2, 3, D)
    hidden = modulate(latent, norm_gain, modulation[0, 0], modulation[0, 1])
    hidden_ctx = modulate(context, norm_gain, modulation[1, 0], modulation[1, 1])
    positions = jnp.arange(LAT, dtype=jnp.int32)
    query_raw = jnp.dot(hidden, w_query, preferred_element_type=jnp.float32).reshape(LAT, HEADS, 2, DK)
    key_raw = jnp.dot(hidden, w_key, preferred_element_type=jnp.float32).reshape(LAT, HEADS, 2, DK)
    ctx_key_raw = jnp.dot(hidden_ctx, w_key, preferred_element_type=jnp.float32).reshape(CTX, HEADS, 2, DK)
    queries = rotate(head_norm(query_raw, query_gain), positions).astype(jnp.bfloat16)
    lat_keys = rotate(head_norm(key_raw, key_gain), positions).astype(jnp.bfloat16)
    ctx_keys = head_norm(ctx_key_raw, key_gain).astype(jnp.bfloat16)
    lat_values = jnp.dot(hidden, w_value, preferred_element_type=jnp.float32).astype(jnp.bfloat16).reshape(LAT, HEADS, DV)
    ctx_values = jnp.dot(hidden_ctx, w_value, preferred_element_type=jnp.float32).astype(jnp.bfloat16).reshape(CTX, HEADS, DV)
    all_keys = jnp.concatenate([ctx_keys, lat_keys], axis=0)
    all_values = jnp.concatenate([ctx_values, lat_values], axis=0)
    block_rows = math.gcd(LAT, 512)
    scaling = DK ** (-0.5)

    def one_head(head_index):
        head_keys = lax.dynamic_index_in_dim(all_keys, head_index, 1, False).astype(jnp.float32)
        head_values = lax.dynamic_index_in_dim(all_values, head_index, 1, False).astype(jnp.float32)
        head_queries = lax.dynamic_index_in_dim(queries, head_index, 1, False).astype(jnp.float32)
        head_queries = head_queries.reshape(LAT // block_rows, block_rows, 2, DK)
        weight_lambda = lax.dynamic_index_in_dim(lambdas, head_index, 0, False)

        def one_block(query_block):
            scores = jnp.einsum('qmd,kmd->qmk', query_block, head_keys) * scaling
            row_peak = lax.optimization_barrier(jnp.max(scores, axis=-1, keepdims=True))
            exponent = jnp.exp(scores - row_peak)
            row_sums = lax.optimization_barrier(jnp.sum(exponent, axis=-1))
            weights = lax.optimization_barrier(exponent.astype(jnp.bfloat16)).astype(jnp.float32)
            blended = jnp.einsum('qmk,kv->qmv', weights, head_values)
            attended = blended[:, 0] / row_sums[:, 0, None] - weight_lambda * blended[:, 1] / row_sums[:, 1, None]
            return head_norm(attended, out_gain)
        return lax.map(one_block, head_queries).reshape(LAT, DV)
    outputs = lax.map(one_head, jnp.arange(HEADS, dtype=jnp.int32))
    head_out = jnp.transpose(outputs, (1, 0, 2)).reshape(LAT, HEADS * DV).astype(jnp.bfloat16)
    mixed_rows = jnp.dot(head_out, w_out, preferred_element_type=jnp.float32)
    return (latent.astype(jnp.float32) + modulation[0, 2] * mixed_rows).astype(jnp.bfloat16)
```

```python
import functools

import jax
import jax.numpy as jnp
import numpy as np
from jax import lax
from jax.experimental import pallas as pl
from jax.experimental.pallas import tpu as pltpu
from jax.sharding import PartitionSpec as P

DK = 64
DV = 128
GRID_W = 64
EPS = 1e-06
LOG2E = 1.4426950408889634
MESH = pl.DeviceIdType.MESH
F32 = jnp.float32
BF16 = jnp.bfloat16


def angle_tables(grid_rows):
    half, quarter = DK // 2, DK // 4
    lane = np.arange(2 * DK) % DK
    inverse = (10000.0 ** (-2.0 * (lane % quarter) / half)).astype(np.float32)
    sign = np.where(lane % half < quarter, -1.0, 1.0).astype(np.float32)
    places = np.concatenate([np.arange(grid_rows), np.arange(GRID_W)]).astype(np.float32)
    angles = (places[:, None] * inverse[None, :]).astype(np.float32).astype(np.float64)
    return np.cos(angles).astype(np.float32), (np.sin(angles) * sign).astype(np.float32)


def kernel(
    nsp,
    ntp,
    latent,
    context,
    part,
    gain,
    w_query,
    w_key,
    w_value,
    query_gain,
    key_gain,
    lambdas,
    out_gain,
    w_out,
    cos_table,
    sin_table,
    out,
    feats,
    weights,
    w_mix,
    shares,
    pairs,
    squares,
    hid,
    proj,
    queries,
    kv,
    peak,
    total,
    blend,
    heads,
    mixed,
    load_sem,
    share_send,
    share_recv,
    pair_send,
    pair_recv,
    x_send,
    x_recv,
    d_send,
    d_recv,
    z_send,
    z_recv,
    o_send,
    o_recv,
    e_send,
    e_recv,
):
    me_sp, me_tp = lax.axis_index("sp"), lax.axis_index("tp")
    core, chip = lax.rem(me_tp, 2), lax.div(me_tp, 2)
    nchip = ntp // 2
    x_last, z_last = nchip // 2, nsp // 2
    partner = me_tp + 1 - 2 * core
    n_lat, cols = latent.shape
    n_ctx = context.shape[0]
    half = n_lat // 2
    offs, sizes = (0, half + n_ctx), (half + n_ctx, half)
    width = cols * ntp

    loads = [
        pltpu.make_async_copy(
            latent.at[pl.ds(0, half)], feats.at[me_tp, pl.ds(0, half)], load_sem.at[0]
        ),
        pltpu.make_async_copy(context, feats.at[me_tp, pl.ds(half, n_ctx)], load_sem.at[1]),
        pltpu.make_async_copy(
            latent.at[pl.ds(half, half)], feats.at[me_tp, pl.ds(offs[1], half)], load_sem.at[2]
        ),
        pltpu.make_async_copy(w_query, weights.at[:, :, pl.ds(0, 128)], load_sem.at[3]),
        pltpu.make_async_copy(w_key, weights.at[:, :, pl.ds(128, 128)], load_sem.at[4]),
        pltpu.make_async_copy(w_value, weights.at[:, :, pl.ds(256, 128)], load_sem.at[5]),
        pltpu.make_async_copy(w_out, w_mix, load_sem.at[6]),
    ]
    for load in loads:
        load.start()

    for at, (c, j) in enumerate(((0, 0), (0, 1), (1, 0), (1, 1), (0, 2))):
        shares[me_sp, :, at * cols : (at + 1) * cols] = part[c, j : j + 1, :]
    peak[...] = jnp.full(peak.shape, -1e30, F32)
    total[...] = jnp.zeros(total.shape, F32)
    blend[...] = jnp.zeros(blend.shape, F32)

    barrier = pltpu.get_barrier_semaphore()

    def greet_sp(k, carry):
        pl.semaphore_signal(
            barrier, 1, device_id={"sp": lax.rem(me_sp + k, nsp)}, device_id_type=MESH
        )
        return carry

    def greet_tp(k, carry):
        pl.semaphore_signal(
            barrier, 1, device_id={"tp": lax.rem(me_tp + k, ntp)}, device_id_type=MESH
        )
        return carry

    lax.fori_loop(1, nsp, greet_sp, 0)
    lax.fori_loop(1, ntp, greet_tp, 0)
    pl.semaphore_wait(barrier, nsp + ntp - 2)

    def share_copy(k, source):
        return pltpu.make_async_remote_copy(
            shares.at[source],
            shares.at[source],
            share_send.at[k],
            share_recv.at[k],
            device_id={"sp": lax.rem(me_sp + k, nsp)},
            device_id_type=MESH,
        )

    def pair_copy(k, source):
        return pltpu.make_async_remote_copy(
            pairs.at[source],
            pairs.at[source],
            pair_send.at[k],
            pair_recv.at[k],
            device_id={"tp": lax.rem(me_tp + k, ntp)},
            device_id_type=MESH,
        )

    def each(first, last, fn):
        def step(k, carry):
            fn(k)
            return carry

        lax.fori_loop(first, last, step, 0)

    each(1, nsp, lambda k: share_copy(k, me_sp).start())

    def place(h):
        return pl.ds(offs[h], sizes[h])

    def rows(h):
        return pl.ds(h * half, half)

    def tp_block(direction, step, which):
        there = chip - step if direction == 0 else chip + step
        return lax.rem(there + nchip, nchip) * 2 + which

    def ring_copy(buf, at, direction, step, h, send, recv):
        block = tp_block(direction, step - 1, core)
        target = me_tp + 2 if direction == 0 else me_tp + ntp - 2
        return pltpu.make_async_remote_copy(
            buf.at[block, at(h)],
            buf.at[block, at(h)],
            send.at[direction, step - 1, h],
            recv.at[direction, step - 1, h],
            device_id={"tp": lax.rem(target, ntp)},
            device_id_type=MESH,
        )

    def ring_arrival(buf, at, direction, step, h, send, recv):
        block = tp_block(direction, step, core)
        return pltpu.make_async_remote_copy(
            buf.at[block, at(h)],
            buf.at[block, at(h)],
            send.at[direction, step - 1, h],
            recv.at[direction, step - 1, h],
            device_id={"tp": partner},
            device_id_type=MESH,
        )

    def mate_copy(buf, at, direction, step, h, send, recv, which):
        block = tp_block(direction, step, which)
        slot = h if step == 0 else 2 + ((step - 1) * 2 + direction) * 2 + h
        return pltpu.make_async_remote_copy(
            buf.at[block, at(h)],
            buf.at[block, at(h)],
            send.at[slot],
            recv.at[slot],
            device_id={"tp": partner},
            device_id_type=MESH,
        )

    def has(direction, step, h, last):
        return step < last or (step == last and direction == h)

    def feature_step(step):
        for h in (0, 1):
            for d in (0, 1):
                if not has(d, step, h, x_last):
                    continue
                ring_arrival(feats, place, d, step, h, x_send, x_recv).wait_recv()
                if has(d, step + 1, h, x_last):
                    ring_copy(feats, place, d, step + 1, h, x_send, x_recv).start()
                mate_copy(feats, place, d, step, h, d_send, d_recv, core).start()

    for h in (0, 1):
        if h == 0:
            loads[0].wait()
            loads[1].wait()
        else:
            loads[2].wait()
        for d in (0, 1):
            ring_copy(feats, place, d, 1, h, x_send, x_recv).start()
        mate_copy(feats, place, 0, 0, h, d_send, d_recv, core).start()

    for step in range(1, x_last - 1):
        feature_step(step)

    each(1, nsp, lambda k: share_copy(k, lax.rem(me_sp + nsp - k, nsp)).wait_recv())
    modulation = jnp.sum(shares[...], axis=0)
    gate = modulation[:, 4 * cols : 5 * cols]
    gains = gain[...]
    pairs[me_tp, :, 0:cols] = modulation[:, 0:cols]
    pairs[me_tp, :, cols : 2 * cols] = gains * (1.0 + modulation[:, cols : 2 * cols])
    pairs[me_tp, :, 2 * cols : 3 * cols] = modulation[:, 2 * cols : 3 * cols]
    pairs[me_tp, :, 3 * cols : 4 * cols] = gains * (1.0 + modulation[:, 3 * cols : 4 * cols])
    each(1, ntp, lambda k: pair_copy(k, me_tp).start())

    for step in range(x_last - 1, x_last + 1):
        feature_step(step)

    for load in loads[3:6]:
        load.wait()
    each(1, ntp, lambda k: pair_copy(k, lax.rem(me_tp + ntp - k, ntp)).wait_recv())

    def z_block(direction, step):
        return lax.rem(me_sp + nsp + (2 * direction - 1) * step, nsp)

    def z_copy(direction, step, h):
        block = z_block(direction, step - 1)
        target = me_sp + 1 if direction == 0 else me_sp + nsp - 1
        return pltpu.make_async_remote_copy(
            kv.at[block, place(h)],
            kv.at[block, place(h)],
            z_send.at[direction, step - 1, h],
            z_recv.at[direction, step - 1, h],
            device_id={"sp": lax.rem(target, nsp)},
            device_id_type=MESH,
        )

    def z_arrival(direction, step, h):
        block = z_block(direction, step)
        target = me_sp + 1 if direction == 0 else me_sp + nsp - 1
        return pltpu.make_async_remote_copy(
            kv.at[block, place(h)],
            kv.at[block, place(h)],
            z_send.at[direction, step - 1, h],
            z_recv.at[direction, step - 1, h],
            device_id={"sp": lax.rem(target, nsp)},
            device_id_type=MESH,
        )

    lane = lax.broadcasted_iota(jnp.int32, (1, 2 * DK), 1)
    first_map = lane < DK
    by_row = lax.rem(lane, DK) < DK // 2
    lower = lax.rem(lane, DK // 2) < DK // 4
    grid_rows = half // GRID_W
    table_rows = nsp * 2 * grid_rows

    def head_norm(x, g):
        squared = x * x
        one = jnp.sum(jnp.where(first_map, squared, 0.0), axis=1, keepdims=True)
        two = jnp.sum(jnp.where(first_map, 0.0, squared), axis=1, keepdims=True)
        scale = jnp.where(
            first_map, lax.rsqrt(one * (1.0 / DK) + EPS), lax.rsqrt(two * (1.0 / DK) + EPS)
        )
        return x * scale * g

    def positions(table, h):
        mine = table[
            pl.ds(pl.multiple_of(me_sp * (2 * grid_rows), 2 * grid_rows), 2 * grid_rows), :
        ]
        columns = table[table_rows : table_rows + GRID_W, :]
        return jnp.concatenate(
            [
                jnp.where(by_row, mine[h * grid_rows + g : h * grid_rows + g + 1, :], columns)
                for g in range(grid_rows)
            ],
            axis=0,
        )

    def turn(x, cosine, sine):
        other = jnp.where(
            lower, pltpu.roll(x, 2 * DK - DK // 4, axis=1), pltpu.roll(x, DK // 4, axis=1)
        )
        return x * cosine + other * sine

    q_gain = jnp.concatenate([query_gain[...], query_gain[...]], axis=1) * (DK**-0.5 * LOG2E)
    k_gain = jnp.concatenate([key_gain[...], key_gain[...]], axis=1)

    def project(h):
        n = sizes[h]
        squares[...] = jnp.zeros(squares.shape, F32)

        def add_squares(b, carry):
            x = feats[b, offs[h] : offs[h] + n, :].astype(F32)
            y = x * x
            squares[0:n, :] += y[:, 0:128] + y[:, 128:256]
            return carry

        lax.fori_loop(0, ntp, add_squares, 0)
        factor = lax.rsqrt(
            jnp.sum(squares[0:n, :], axis=1, keepdims=True) * (1.0 / width) + EPS
        )
        squares[0:n, :] = jnp.broadcast_to(factor, (n, 128))
        proj[...] = jnp.zeros(proj.shape, F32)

        def add_block(b, carry):
            x = feats[b, offs[h] : offs[h] + half, :].astype(F32)
            f = jnp.concatenate([squares[0:half, :], squares[0:half, :]], axis=1)
            hid[0:half, :] = (
                x * f * pairs[b, :, cols : 2 * cols] + pairs[b, :, 0:cols]
            ).astype(BF16)
            if n > half:
                x = feats[b, offs[h] + half : offs[h] + n, :].astype(F32)
                f = jnp.concatenate([squares[half:n, :], squares[half:n, :]], axis=1)
                hid[half:n, :] = (
                    x * f * pairs[b, :, 3 * cols : 4 * cols] + pairs[b, :, 2 * cols : 3 * cols]
                ).astype(BF16)
            proj[0:n, :] += jnp.dot(hid[0:n, :], weights[b], preferred_element_type=F32)
            return carry

        lax.fori_loop(0, ntp, add_block, 0, unroll=2)
        cosine, sine = positions(cos_table, h), positions(sin_table, h)
        q = turn(head_norm(proj[0:half, 0:128], q_gain), cosine, sine)
        queries[h] = jnp.where(first_map, q, 0.0).astype(BF16)
        queries[2 + h] = jnp.where(first_map, 0.0, q).astype(BF16)
        k = turn(head_norm(proj[0:half, 128:256], k_gain), cosine, sine)
        kv[me_sp, offs[h] : offs[h] + half, 0:128] = k.astype(BF16)
        if n > half:
            kv[me_sp, offs[h] + half : offs[h] + n, 0:128] = head_norm(
                proj[half:n, 128:256], k_gain
            ).astype(BF16)
        kv[me_sp, offs[h] : offs[h] + n, 128:256] = proj[0:n, 256:384].astype(BF16)

    def mates(step_h, buf, at, send, recv):
        for step in range(0, x_last + 1):
            for d in (0, 1):
                if step == 0 and d == 1:
                    continue
                if step and not has(d, step, step_h, x_last):
                    continue
                mate_copy(buf, at, d, step, step_h, send, recv, 1 - core).wait_recv()

    for h in (0, 1):
        mates(h, feats, place, d_send, d_recv)
        project(h)
        for d in (0, 1):
            z_copy(d, 1, h).start()

    def absorb(block, h, chunks):
        n = sizes[h]
        keys = kv[block, offs[h] : offs[h] + n, 0:128]
        values = kv[block, offs[h] : offs[h] + n, 128:256]
        for c in chunks:
            scores = lax.dot_general(
                keys, queries[c], (((1,), (1,)), ((), ())), preferred_element_type=F32
            )
            old = peak[c]
            new = jnp.maximum(old, jnp.max(scores, axis=0, keepdims=True))
            expo = jnp.exp2(scores - new)
            rescale = jnp.exp2(old - new)
            total[c] = total[c] * rescale + jnp.sum(expo, axis=0, keepdims=True)
            blend[c] = blend[c] * rescale + lax.dot_general(
                values, expo.astype(BF16), (((0,), (0,)), ((), ())), preferred_element_type=F32
            )
            peak[c] = new

    for h in (0, 1):
        absorb(me_sp, h, range(4))

    def z_step(step, carry):
        for h in (0, 1):
            for d in (0, 1):
                z_arrival(d, step, h).wait_recv()
                if d == h:
                    z_copy(d, step + 1, h).start()
                else:

                    @pl.when(step < z_last - 1)
                    def _():
                        z_copy(d, step + 1, h).start()

            def both(d, inner):
                absorb(z_block(d, step), h, range(4))
                return inner

            lax.fori_loop(0, 2, both, 0)
        return carry

    lax.fori_loop(1, z_last, z_step, 0)
    for h in (0, 1):
        z_arrival(h, z_last, h).wait_recv()

    loads[6].wait()
    weight = lambdas[0]
    for h in (0, 1):
        for piece in (0, 1):
            absorb(z_block(piece, z_last), piece, (h, 2 + h))
        attended = blend[h] / total[h] - weight * (blend[2 + h] / total[2 + h])
        scale = lax.rsqrt(jnp.sum(attended * attended, axis=0, keepdims=True) * (1.0 / DV) + EPS)
        heads[me_tp, h * half : (h + 1) * half, :] = (
            jnp.transpose(attended * scale) * out_gain[...]
        ).astype(BF16)
        for d in (0, 1):
            ring_copy(heads, rows, d, 1, h, o_send, o_recv).start()
        mate_copy(heads, rows, 0, 0, h, e_send, e_recv, core).start()

    def mix(direction, step, h):
        mate_copy(heads, rows, direction, step, h, e_send, e_recv, 1 - core).wait_recv()
        first = tp_block(direction, step, 0)
        both = jnp.concatenate(
            [
                heads[first, h * half : (h + 1) * half, :],
                heads[first + 1, h * half : (h + 1) * half, :],
            ],
            axis=1,
        )
        piece = jnp.dot(both, w_mix[lax.div(first, 2)], preferred_element_type=F32)
        if step == 0:
            mixed[h * half : (h + 1) * half, :] = piece
        else:
            mixed[h * half : (h + 1) * half, :] += piece

    for h in (0, 1):
        mix(0, 0, h)
    for step in range(1, x_last + 1):
        for h in (0, 1):
            here = [d for d in (0, 1) if has(d, step, h, x_last)]
            for d in here:
                ring_arrival(heads, rows, d, step, h, o_send, o_recv).wait_recv()
                if has(d, step + 1, h, x_last):
                    ring_copy(heads, rows, d, step + 1, h, o_send, o_recv).start()
                mate_copy(heads, rows, d, step, h, e_send, e_recv, core).start()
            for d in here:
                mix(d, step, h)
            if step == x_last:
                mine = feats[me_tp, offs[h] : offs[h] + half, :].astype(F32)
                out[h * half : (h + 1) * half, :] = (
                    mine + gate * mixed[h * half : (h + 1) * half, :]
                ).astype(BF16)

    each(1, nsp, lambda k: share_copy(k, me_sp).wait_send())
    each(1, ntp, lambda k: pair_copy(k, me_tp).wait_send())
    for buf, at, send, recv, own_send, own_recv in (
        (feats, place, x_send, x_recv, d_send, d_recv),
        (heads, rows, o_send, o_recv, e_send, e_recv),
    ):
        for step in range(0, x_last + 1):
            for d in (0, 1):
                for h in (0, 1):
                    if step and has(d, step, h, x_last):
                        ring_copy(buf, at, d, step, h, send, recv).wait_send()
                    if (step and has(d, step, h, x_last)) or (step == 0 and d == 0):
                        mate_copy(buf, at, d, step, h, own_send, own_recv, core).wait_send()

    def z_sent(step, carry):
        for h in (0, 1):
            for d in (0, 1):
                z_copy(d, step, h).wait_send()
        return carry

    lax.fori_loop(1, z_last, z_sent, 0)
    for h in (0, 1):
        z_copy(h, z_last, h).wait_send()


def local(
    latent,
    context,
    conditions,
    mod_weight,
    norm_gain,
    w_query,
    w_key,
    w_value,
    query_gain,
    key_gain,
    lambdas,
    out_gain,
    w_out,
):
    nsp, ntp = lax.axis_size("sp"), lax.axis_size("tp")
    n_lat, cols = latent.shape
    n_ctx = context.shape[0]
    block = n_lat + n_ctx
    half = n_lat // 2
    nchip = ntp // 2
    activated = jax.nn.silu(conditions).astype(BF16)
    part = jnp.einsum("ci,ijn->cjn", activated, mod_weight, preferred_element_type=F32)
    cosine, sine = angle_tables(nsp * n_lat // GRID_W)
    vmem = pl.BlockSpec(memory_space=pltpu.VMEM)
    smem = pl.BlockSpec(memory_space=pltpu.SMEM)
    hbm = pl.BlockSpec(memory_space=pl.ANY)
    dma = pltpu.SemaphoreType.DMA
    return pl.pallas_call(
        functools.partial(kernel, nsp, ntp),
        out_shape=jax.ShapeDtypeStruct((n_lat, cols), BF16),
        in_specs=[hbm, hbm, vmem, vmem, hbm, hbm, hbm, vmem, vmem, smem, vmem, hbm, vmem, vmem],
        out_specs=vmem,
        scratch_shapes=[
            pltpu.VMEM((ntp, block, cols), BF16),
            pltpu.VMEM((ntp, cols, 3 * DV), BF16),
            pltpu.VMEM((nchip, 2 * DV, cols), BF16),
            pltpu.VMEM((nsp, 1, 5 * cols), F32),
            pltpu.VMEM((ntp, 1, 4 * cols), F32),
            pltpu.VMEM((half + n_ctx, 128), F32),
            pltpu.VMEM((half + n_ctx, cols), BF16),
            pltpu.VMEM((half + n_ctx, 3 * DV), F32),
            pltpu.VMEM((4, half, 2 * DK), BF16),
            pltpu.VMEM((nsp, block, 2 * DK + DV), BF16),
            pltpu.VMEM((4, 1, half), F32),
            pltpu.VMEM((4, 1, half), F32),
            pltpu.VMEM((4, DV, half), F32),
            pltpu.VMEM((ntp, n_lat, DV), BF16),
            pltpu.VMEM((n_lat, cols), F32),
            dma((7,)),
            dma((nsp,)),
            dma((nsp,)),
            dma((ntp,)),
            dma((ntp,)),
            dma((2, nchip // 2, 2)),
            dma((2, nchip // 2, 2)),
            dma((2 + 2 * nchip,)),
            dma((2 + 2 * nchip,)),
            dma((2, nsp // 2, 2)),
            dma((2, nsp // 2, 2)),
            dma((2, nchip // 2, 2)),
            dma((2, nchip // 2, 2)),
            dma((2 + 2 * nchip,)),
            dma((2 + 2 * nchip,)),
        ],
        compiler_params=pltpu.CompilerParams(collective_id=0, has_side_effects=True),
    )(
        latent,
        context,
        part,
        norm_gain[None],
        w_query.reshape(ntp, cols, DV),
        w_key.reshape(ntp, cols, DV),
        w_value.reshape(ntp, cols, DV),
        query_gain[None],
        key_gain[None],
        lambdas,
        out_gain[None],
        w_out.reshape(nchip, 2 * DV, cols),
        jnp.asarray(cosine),
        jnp.asarray(sine),
    )


def solution(mesh):
    in_specs = (
        P(("grp", "sp"), "tp"),
        P(("grp", "sp"), "tp"),
        P("grp", "sp"),
        P("sp", None, "tp"),
        P("tp"),
        P(None, "tp"),
        P(None, "tp"),
        P(None, "tp"),
        P(),
        P(),
        P("tp"),
        P(),
        P(None, "tp"),
    )
    out_specs = P(("grp", "sp"), "tp")
    return jax.shard_map(local, mesh=mesh, in_specs=in_specs, out_specs=out_specs, check_vma=False)
```

```python
import functools

import jax
import jax.numpy as jnp
import numpy as np
from jax import lax
from jax.experimental import pallas as pl
from jax.experimental.pallas import tpu as pltpu
from jax.sharding import PartitionSpec as P

DK = 64
DV = 128
GRID_W = 64
EPS = 1e-06
LOG2E = 1.4426950408889634
MESH = pl.DeviceIdType.MESH
F32 = jnp.float32
BF16 = jnp.bfloat16


def angle_tables(grid_rows):
    half, quarter = DK // 2, DK // 4
    lane = np.arange(2 * DK) % DK
    inverse = (10000.0 ** (-2.0 * (lane % quarter) / half)).astype(np.float32)
    sign = np.where(lane % half < quarter, -1.0, 1.0).astype(np.float32)
    places = np.concatenate([np.arange(grid_rows), np.arange(GRID_W)]).astype(np.float32)
    angles = (places[:, None] * inverse[None, :]).astype(np.float32).astype(np.float64)
    return np.cos(angles).astype(np.float32), (np.sin(angles) * sign).astype(np.float32)


def kernel(
    nsp,
    ntp,
    latent,
    context,
    part,
    gain,
    w_query,
    w_key,
    w_value,
    query_gain,
    key_gain,
    lambdas,
    out_gain,
    w_out,
    cos_table,
    sin_table,
    out,
    feats,
    weights,
    w_mix,
    shares,
    pairs,
    factors,
    proj,
    queries,
    kv,
    peak,
    total,
    blend,
    heads,
    mixed,
    load_sem,
    share_send,
    share_recv,
    pair_send,
    pair_recv,
    x_send,
    x_recv,
    d_send,
    d_recv,
    z_send,
    z_recv,
    o_send,
    o_recv,
    e_send,
    e_recv,
):
    me_sp, me_tp = lax.axis_index("sp"), lax.axis_index("tp")
    core, chip = lax.rem(me_tp, 2), lax.div(me_tp, 2)
    nchip = ntp // 2
    x_last, z_last = nchip // 2, nsp // 2
    partner = me_tp + 1 - 2 * core
    n_lat, cols = latent.shape
    n_ctx = context.shape[0]
    half, quarter = n_lat // 2, n_lat // 4
    width = cols * ntp
    lead = GRID_W
    chunks = (
        (0, lead, n_ctx, 0),
        (lead + n_ctx, quarter, 0, lead),
        (lead + n_ctx + quarter, quarter, 0, lead + quarter),
        (lead + n_ctx + 2 * quarter, n_lat - lead - 2 * quarter, 0, lead + 2 * quarter),
    )
    pieces = range(4)

    loads = []

    def load(src, dst):
        loads.append(pltpu.make_async_copy(src, dst, load_sem.at[len(loads)]))
        loads[-1].start()

    load(latent.at[pl.ds(0, lead)], feats.at[me_tp, pl.ds(0, lead)])
    load(context, feats.at[me_tp, pl.ds(lead, n_ctx)])
    load(latent.at[pl.ds(lead, n_lat - lead)], feats.at[me_tp, pl.ds(lead + n_ctx, n_lat - lead)])
    load(w_query, weights.at[:, :, pl.ds(0, 128)])
    load(w_key, weights.at[:, :, pl.ds(128, 128)])
    load(w_value, weights.at[:, :, pl.ds(256, 128)])
    load(w_out, w_mix)

    for at, (c, j) in enumerate(((0, 0), (0, 1), (1, 0), (1, 1), (0, 2))):
        shares[me_sp, :, at * cols : (at + 1) * cols] = part[c, j : j + 1, :]

    barrier = pltpu.get_barrier_semaphore()

    def each(first, last, fn):
        def step(k, carry):
            fn(k)
            return carry

        lax.fori_loop(first, last, step, 0)

    def greet(axis, target):
        pl.semaphore_signal(barrier, 1, device_id={axis: target}, device_id_type=MESH)

    each(1, nsp, lambda k: greet("sp", lax.rem(me_sp + k, nsp)))
    each(1, ntp, lambda k: greet("tp", lax.rem(me_tp + k, ntp)))
    peak[...] = jnp.full(peak.shape, -1e30, F32)
    total[...] = jnp.zeros(total.shape, F32)
    blend[...] = jnp.zeros(blend.shape, F32)
    pl.semaphore_wait(barrier, nsp + ntp - 2)

    def share_copy(k, source):
        return pltpu.make_async_remote_copy(
            shares.at[source],
            shares.at[source],
            share_send.at[k],
            share_recv.at[k],
            device_id={"sp": lax.rem(me_sp + k, nsp)},
            device_id_type=MESH,
        )

    def pair_copy(k, source):
        return pltpu.make_async_remote_copy(
            pairs.at[source],
            pairs.at[source],
            pair_send.at[k],
            pair_recv.at[k],
            device_id={"tp": lax.rem(me_tp + k, ntp)},
            device_id_type=MESH,
        )

    each(1, nsp, lambda k: share_copy(k, me_sp).start())

    def place(c):
        return pl.ds(chunks[c][0], chunks[c][1] + chunks[c][2])

    def rows(c):
        return pl.ds(c * quarter, quarter)

    def tp_block(direction, step, which):
        return lax.rem(chip + nchip + (2 * direction - 1) * step, nchip) * 2 + which

    def z_block(direction, step):
        return lax.rem(me_sp + nsp + (2 * direction - 1) * step, nsp)

    class Ring:
        def __init__(self, buf, at, block, target, send, recv, last):
            self.buf, self.at, self.block, self.target = buf, at, block, target
            self.send, self.recv, self.last = send, recv, last

        def copy(self, direction, step, c, back=1):
            where = self.buf.at[self.block(direction, step - back), self.at(c)]
            return pltpu.make_async_remote_copy(
                where,
                where,
                self.send.at[direction, step - 1, c],
                self.recv.at[direction, step - 1, c],
                device_id=self.target(direction),
                device_id_type=MESH,
            )

        def begin(self, c):
            for d in (0, 1):
                self.copy(d, 1, c).start()

        def advance(self, step, c, after=None):
            for d in (0, 1):
                self.copy(d, step, c, back=0).wait_recv()
                if d == c % 2:
                    self.copy(d, step + 1, c).start()
                else:

                    @pl.when(step < self.last - 1)
                    def _():
                        self.copy(d, step + 1, c).start()

                if after is not None:
                    after(d, step, c)

        def finish(self, c, after=None):
            self.copy(c % 2, self.last, c, back=0).wait_recv()
            if after is not None:
                after(c % 2, self.last, c)

        def sent(self):
            def step_sent(step):
                for c in pieces:
                    for d in (0, 1):
                        self.copy(d, step, c).wait_send()

            each(1, self.last, step_sent)
            for c in pieces:
                self.copy(c % 2, self.last, c).wait_send()

    def tp_target(direction):
        return {"tp": lax.rem(me_tp + (2 if direction == 0 else ntp - 2), ntp)}

    def sp_target(direction):
        return {"sp": lax.rem(me_sp + (1 if direction == 0 else nsp - 1), nsp)}

    def own_block(direction, step):
        return tp_block(direction, step, core)

    x_ring = Ring(feats, place, own_block, tp_target, x_send, x_recv, x_last)
    z_ring = Ring(kv, place, z_block, sp_target, z_send, z_recv, z_last)
    o_ring = Ring(heads, rows, own_block, tp_target, o_send, o_recv, x_last)

    class Mate:
        def __init__(self, buf, at, send, recv):
            self.buf, self.at, self.send, self.recv = buf, at, send, recv

        def copy(self, direction, step, c, which):
            own = isinstance(step, int) and step == 0
            slot = c if own else 4 + ((step - 1) * 2 + direction) * 4 + c
            where = self.buf.at[tp_block(direction, step, which), self.at(c)]
            return pltpu.make_async_remote_copy(
                where,
                where,
                self.send.at[slot],
                self.recv.at[slot],
                device_id={"tp": partner},
                device_id_type=MESH,
            )

        def give(self, direction, step, c):
            self.copy(direction, step, c, core).start()

        def every(self, c, fn):
            fn(0, 0, c)

            def step_fn(step):
                for d in (0, 1):
                    fn(d, step, c)

            each(1, x_last, step_fn)
            fn(c % 2, x_last, c)

    x_mate = Mate(feats, place, d_send, d_recv)
    o_mate = Mate(heads, rows, e_send, e_recv)

    def begin_features(c):
        x_ring.begin(c)
        x_mate.give(0, 0, c)

    loads[0].wait()
    loads[1].wait()
    begin_features(0)
    loads[2].wait()
    begin_features(1)

    def first_features(step):
        x_ring.advance(step, 0, x_mate.give)
        x_ring.advance(step, 1, x_mate.give)

    def later_features(step):
        x_ring.advance(step, 2, x_mate.give)
        x_ring.advance(step, 3, x_mate.give)

    each(1, x_last, first_features)
    begin_features(2)
    begin_features(3)
    x_ring.finish(0, x_mate.give)
    x_ring.finish(1, x_mate.give)

    def measure(c):
        at, n = chunks[c][0], chunks[c][1] + chunks[c][2]
        x_mate.every(c, lambda d, step, c: x_mate.copy(d, step, c, 1 - core).wait_recv())

        def add_squares(b, carry):
            x = feats[b, at : at + n, :].astype(F32)
            y = x * x
            return carry + y[:, 0:128] + y[:, 128:256]

        squares = lax.fori_loop(0, ntp, add_squares, jnp.zeros((n, 128), F32))
        factor = lax.rsqrt(jnp.sum(squares, axis=1, keepdims=True) * (1.0 / width) + EPS)
        factors[at : at + n, :] = jnp.broadcast_to(factor, (n, 128))

    measure(0)
    measure(1)
    each(1, nsp, lambda k: share_copy(k, lax.rem(me_sp + nsp - k, nsp)).wait_recv())
    modulation = jnp.sum(shares[...], axis=0)
    gate = modulation[:, 4 * cols : 5 * cols]
    gains = gain[...]
    pairs[me_tp, :, 0:cols] = modulation[:, 0:cols]
    pairs[me_tp, :, cols : 2 * cols] = gains * (1.0 + modulation[:, cols : 2 * cols])
    pairs[me_tp, :, 2 * cols : 3 * cols] = modulation[:, 2 * cols : 3 * cols]
    pairs[me_tp, :, 3 * cols : 4 * cols] = gains * (1.0 + modulation[:, 3 * cols : 4 * cols])
    each(1, ntp, lambda k: pair_copy(k, me_tp).start())
    later_features(1)
    for one in loads[3:6]:
        one.wait()
    each(1, ntp, lambda k: pair_copy(k, lax.rem(me_tp + ntp - k, ntp)).wait_recv())

    lane = lax.broadcasted_iota(jnp.int32, (1, 2 * DK), 1)
    first_map = lane < DK
    by_row = lax.rem(lane, DK) < DK // 2
    lower = lax.rem(lane, DK // 2) < DK // 4
    grid_rows = n_lat // GRID_W
    table_rows = nsp * grid_rows

    def head_norm(x, g):
        squared = x * x
        one = jnp.sum(jnp.where(first_map, squared, 0.0), axis=1, keepdims=True)
        two = jnp.sum(jnp.where(first_map, 0.0, squared), axis=1, keepdims=True)
        scale = jnp.where(
            first_map, lax.rsqrt(one * (1.0 / DK) + EPS), lax.rsqrt(two * (1.0 / DK) + EPS)
        )
        return x * scale * g

    def positions(table, first, n):
        mine = table[pl.ds(pl.multiple_of(me_sp * grid_rows, grid_rows), grid_rows), :]
        columns = table[table_rows : table_rows + GRID_W, :]
        return jnp.concatenate(
            [
                jnp.where(by_row, mine[g : g + 1, :], columns)
                for g in range(first // GRID_W, (first + n) // GRID_W)
            ],
            axis=0,
        )

    def turn(x, cosine, sine):
        other = jnp.where(
            lower, pltpu.roll(x, 2 * DK - DK // 4, axis=1), pltpu.roll(x, DK // 4, axis=1)
        )
        return x * cosine + other * sine

    q_gain = jnp.concatenate([query_gain[...], query_gain[...]], axis=1) * (DK**-0.5 * LOG2E)
    k_gain = jnp.concatenate([key_gain[...], key_gain[...]], axis=1)

    def project(c):
        at, n_here, n_more, first = chunks[c]
        n = n_here + n_more
        proj[0:n, :] = jnp.zeros((n, 3 * DV), F32)

        def modulated(b, start, count, column):
            x = feats[b, at + start : at + start + count, :].astype(F32)
            f = factors[at + start : at + start + count, :]
            f = jnp.concatenate([f, f], axis=1)
            shift = pairs[b, :, column * cols : (column + 1) * cols]
            scale = pairs[b, :, (column + 1) * cols : (column + 2) * cols]
            return (x * f * scale + shift).astype(BF16)

        def add_block(b, carry):
            x = modulated(b, 0, n_here, 0)
            if n_more:
                x = jnp.concatenate([x, modulated(b, n_here, n_more, 2)], axis=0)
            proj[0:n, :] += jnp.dot(x, weights[b], preferred_element_type=F32)
            return carry

        lax.fori_loop(0, ntp, add_block, 0, unroll=4)
        cosine, sine = positions(cos_table, first, n_here), positions(sin_table, first, n_here)
        k = turn(head_norm(proj[0:n_here, 128:256], k_gain), cosine, sine)
        kv[me_sp, at : at + n_here, 0:128] = k.astype(BF16)
        if n_more:
            kv[me_sp, at + n_here : at + n, 0:128] = head_norm(
                proj[n_here:n, 128:256], k_gain
            ).astype(BF16)
        kv[me_sp, at : at + n, 128:256] = proj[0:n, 256:384].astype(BF16)
        q = turn(head_norm(proj[0:n_here, 0:128], q_gain), cosine, sine)
        queries[0, first : first + n_here, :] = jnp.where(first_map, q, 0.0).astype(BF16)
        queries[1, first : first + n_here, :] = jnp.where(first_map, 0.0, q).astype(BF16)
        z_ring.begin(c)

    def absorb(parts, h):
        for m in (0, 1):
            i = 2 * m + h
            q = queries[m, h * half : (h + 1) * half, :]
            scores = [
                lax.dot_general(
                    kv[block, chunks[c][0] : chunks[c][0] + chunks[c][1] + chunks[c][2], 0:128],
                    q,
                    (((1,), (1,)), ((), ())),
                    preferred_element_type=F32,
                )
                for block, c in parts
            ]
            old = peak[i]
            new = old
            for s in scores:
                new = jnp.maximum(new, jnp.max(s, axis=0, keepdims=True))
            rescale = jnp.exp2(old - new)
            summed, mixture = total[i] * rescale, blend[i] * rescale
            for (block, c), s in zip(parts, scores):
                expo = jnp.exp2(s - new)
                summed += jnp.sum(expo, axis=0, keepdims=True)
                mixture += lax.dot_general(
                    kv[block, chunks[c][0] : chunks[c][0] + chunks[c][1] + chunks[c][2], 128:256],
                    expo.astype(BF16),
                    (((0,), (0,)), ((), ())),
                    preferred_element_type=F32,
                )
            total[i], blend[i], peak[i] = summed, mixture, new

    def absorb_step(step, c):
        for h in (0, 1):
            absorb([(z_block(0, step), c), (z_block(1, step), c)], h)

    def z_step(step, c):
        z_ring.advance(step, c)
        absorb_step(step, c)

    project(0)
    project(1)
    later_features(2)
    later_features(3)
    z_ring.advance(1, 0)
    z_ring.advance(1, 1)
    x_ring.finish(2, x_mate.give)
    x_ring.finish(3, x_mate.give)
    measure(2)
    project(2)
    z_ring.advance(2, 0)
    z_ring.advance(2, 1)
    measure(3)
    project(3)
    z_ring.advance(3, 0)
    z_ring.advance(3, 1)
    for h in (0, 1):
        absorb([(me_sp, 0), (me_sp, 1)], h)
    for h in (0, 1):
        absorb([(me_sp, 2), (me_sp, 3)], h)

    def mingled(step):
        z_step(step, 2)
        z_step(step, 3)
        z_ring.advance(step + 3, 0)
        absorb_step(step, 0)
        z_ring.advance(step + 3, 1)
        absorb_step(step, 1)

    gap = 3
    each(1, z_last - gap, mingled)
    z_ring.finish(0)
    z_ring.finish(1)

    def trailing(step):
        z_step(step, 2)
        absorb_step(step, 0)
        z_step(step, 3)
        absorb_step(step, 1)

    each(z_last - gap, z_last, trailing)
    for h in (0, 1):
        absorb([(z_block(0, z_last), 0), (z_block(1, z_last), 1)], h)
    z_ring.finish(2)
    z_ring.finish(3)

    loads[6].wait()
    weight = lambdas[0]
    for h in (0, 1):
        absorb([(z_block(0, z_last), 2), (z_block(1, z_last), 3)], h)
        attended = blend[h] / total[h] - weight * (blend[2 + h] / total[2 + h])
        scale = lax.rsqrt(jnp.sum(attended * attended, axis=0, keepdims=True) * (1.0 / DV) + EPS)
        heads[me_tp, h * half : (h + 1) * half, :] = (
            jnp.transpose(attended * scale) * out_gain[...]
        ).astype(BF16)
        for c in (2 * h, 2 * h + 1):
            o_ring.begin(c)
            o_mate.give(0, 0, c)

    def mix(direction, step, c):
        o_mate.copy(direction, step, c, 1 - core).wait_recv()
        first = tp_block(direction, step, 0)
        at = c * quarter
        both = jnp.concatenate(
            [heads[first, at : at + quarter, :], heads[first + 1, at : at + quarter, :]], axis=1
        )
        piece = jnp.dot(both, w_mix[lax.div(first, 2)], preferred_element_type=F32)
        if isinstance(step, int) and step == 0:
            mixed[at : at + quarter, :] = piece
        else:
            mixed[at : at + quarter, :] += piece

    for c in pieces:
        mix(0, 0, c)

    def out_step(step):
        for c in pieces:
            o_ring.advance(step, c, o_mate.give)
        for c in pieces:
            for d in (0, 1):
                mix(d, step, c)

    each(1, x_last, out_step)
    for c in pieces:
        o_ring.finish(c, o_mate.give)
    for c in pieces:
        mix(c % 2, x_last, c)
        at = c * quarter
        for start, count in ((at, lead), (at + lead, quarter - lead)):
            shift = 0 if start < lead else n_ctx
            mine = feats[me_tp, start + shift : start + shift + count, :].astype(F32)
            out[start : start + count, :] = (
                mine + gate * mixed[start : start + count, :]
            ).astype(BF16)

    each(1, nsp, lambda k: share_copy(k, me_sp).wait_send())
    each(1, ntp, lambda k: pair_copy(k, me_tp).wait_send())
    for ring in (x_ring, z_ring, o_ring):
        ring.sent()
    for mate in (x_mate, o_mate):
        for c in pieces:
            mate.every(c, lambda d, step, c: mate.copy(d, step, c, core).wait_send())


def local(
    latent,
    context,
    conditions,
    mod_weight,
    norm_gain,
    w_query,
    w_key,
    w_value,
    query_gain,
    key_gain,
    lambdas,
    out_gain,
    w_out,
):
    nsp, ntp = lax.axis_size("sp"), lax.axis_size("tp")
    n_lat, cols = latent.shape
    n_ctx = context.shape[0]
    block = n_lat + n_ctx
    half = n_lat // 2
    nchip = ntp // 2
    activated = jax.nn.silu(conditions).astype(BF16)
    part = jnp.einsum("ci,ijn->cjn", activated, mod_weight, preferred_element_type=F32)
    cosine, sine = angle_tables(nsp * n_lat // GRID_W)
    vmem = pl.BlockSpec(memory_space=pltpu.VMEM)
    smem = pl.BlockSpec(memory_space=pltpu.SMEM)
    hbm = pl.BlockSpec(memory_space=pl.ANY)
    dma = pltpu.SemaphoreType.DMA
    return pl.pallas_call(
        functools.partial(kernel, nsp, ntp),
        out_shape=jax.ShapeDtypeStruct((n_lat, cols), BF16),
        in_specs=[hbm, hbm, vmem, vmem, hbm, hbm, hbm, vmem, vmem, smem, vmem, hbm, vmem, vmem],
        out_specs=vmem,
        scratch_shapes=[
            pltpu.VMEM((ntp, block, cols), BF16),
            pltpu.VMEM((ntp, cols, 3 * DV), BF16),
            pltpu.VMEM((nchip, 2 * DV, cols), BF16),
            pltpu.VMEM((nsp, 1, 5 * cols), F32),
            pltpu.VMEM((ntp, 1, 4 * cols), F32),
            pltpu.VMEM((block, 128), F32),
            pltpu.VMEM((block, 3 * DV), F32),
            pltpu.VMEM((2, n_lat, 2 * DK), BF16),
            pltpu.VMEM((nsp, block, 2 * DK + DV), BF16),
            pltpu.VMEM((4, 1, half), F32),
            pltpu.VMEM((4, 1, half), F32),
            pltpu.VMEM((4, DV, half), F32),
            pltpu.VMEM((ntp, n_lat, DV), BF16),
            pltpu.VMEM((n_lat, cols), F32),
            dma((7,)),
            dma((nsp,)),
            dma((nsp,)),
            dma((ntp,)),
            dma((ntp,)),
            dma((2, nchip // 2, 4)),
            dma((2, nchip // 2, 4)),
            dma((4 + 4 * nchip,)),
            dma((4 + 4 * nchip,)),
            dma((2, nsp // 2, 4)),
            dma((2, nsp // 2, 4)),
            dma((2, nchip // 2, 4)),
            dma((2, nchip // 2, 4)),
            dma((4 + 4 * nchip,)),
            dma((4 + 4 * nchip,)),
        ],
        compiler_params=pltpu.CompilerParams(collective_id=0, has_side_effects=True),
    )(
        latent,
        context,
        part,
        norm_gain[None],
        w_query.reshape(ntp, cols, DV),
        w_key.reshape(ntp, cols, DV),
        w_value.reshape(ntp, cols, DV),
        query_gain[None],
        key_gain[None],
        lambdas,
        out_gain[None],
        w_out.reshape(nchip, 2 * DV, cols),
        jnp.asarray(cosine),
        jnp.asarray(sine),
    )


def solution(mesh):
    in_specs = (
        P(("grp", "sp"), "tp"),
        P(("grp", "sp"), "tp"),
        P("grp", "sp"),
        P("sp", None, "tp"),
        P("tp"),
        P(None, "tp"),
        P(None, "tp"),
        P(None, "tp"),
        P(),
        P(),
        P("tp"),
        P(),
        P(None, "tp"),
    )
    out_specs = P(("grp", "sp"), "tp")
    return jax.shard_map(local, mesh=mesh, in_specs=in_specs, out_specs=out_specs, check_vma=False)
```

```python
import functools

import jax
import jax.numpy as jnp
import numpy as np
from jax import lax
from jax.experimental import pallas as pl
from jax.experimental.pallas import tpu as pltpu
from jax.sharding import PartitionSpec as P

DK = 64
DV = 128
GRID_W = 64
EPS = 1e-06
LOG2E = 1.4426950408889634
MESH = pl.DeviceIdType.MESH
F32 = jnp.float32
BF16 = jnp.bfloat16


def angle_tables(grid_rows):
    half, quarter = DK // 2, DK // 4
    lane = np.arange(2 * DK) % DK
    inverse = (10000.0 ** (-2.0 * (lane % quarter) / half)).astype(np.float32)
    sign = np.where(lane % half < quarter, -1.0, 1.0).astype(np.float32)
    places = np.concatenate([np.arange(grid_rows), np.arange(GRID_W)]).astype(np.float32)
    angles = (places[:, None] * inverse[None, :]).astype(np.float32).astype(np.float64)
    return np.cos(angles).astype(np.float32), (np.sin(angles) * sign).astype(np.float32)


def kernel(
    nsp,
    ntp,
    latent,
    context,
    conditions,
    mod_weight,
    gain,
    w_query,
    w_key,
    w_value,
    query_gain,
    key_gain,
    lambdas,
    out_gain,
    w_out,
    cos_table,
    sin_table,
    out,
    feats,
    w_mod,
    weights,
    w_mix,
    shares,
    pairs,
    factors,
    proj,
    queries,
    kv,
    peak,
    total,
    blend,
    heads,
    mixed,
    load_sem,
    share_send,
    share_recv,
    pair_send,
    pair_recv,
    x_send,
    x_recv,
    d_send,
    d_recv,
    z_send,
    z_recv,
    o_send,
    o_recv,
    e_send,
    e_recv,
):
    me_sp, me_tp = lax.axis_index("sp"), lax.axis_index("tp")
    core, chip = lax.rem(me_tp, 2), lax.div(me_tp, 2)
    nchip = ntp // 2
    x_last, z_last = nchip // 2, nsp // 2
    partner = me_tp + 1 - 2 * core
    n_lat, cols = latent.shape
    n_ctx = context.shape[0]
    half, quarter = n_lat // 2, n_lat // 4
    width = cols * ntp
    lead = GRID_W
    chunks = (
        (0, lead, n_ctx, 0),
        (lead + n_ctx, quarter, 0, lead),
        (lead + n_ctx + quarter, quarter, 0, lead + quarter),
        (lead + n_ctx + 2 * quarter, n_lat - lead - 2 * quarter, 0, lead + 2 * quarter),
    )
    pieces = range(4)

    barrier = pltpu.get_barrier_semaphore()

    def each(first, last, fn):
        def step(k, carry):
            fn(k)
            return carry

        lax.fori_loop(first, last, step, 0)

    def greet(axis, target):
        pl.semaphore_signal(barrier, 1, device_id={axis: target}, device_id_type=MESH)

    each(1, ntp, lambda k: greet("tp", lax.rem(me_tp + k, ntp)))
    each(1, nsp, lambda k: greet("sp", lax.rem(me_sp + k, nsp)))

    loads = []

    def load(src, dst):
        loads.append(pltpu.make_async_copy(src, dst, load_sem.at[len(loads)]))
        loads[-1].start()

    load(latent.at[pl.ds(0, lead)], feats.at[me_tp, pl.ds(0, lead)])
    load(context, feats.at[me_tp, pl.ds(lead, n_ctx)])
    load(latent.at[pl.ds(lead, n_lat - lead)], feats.at[me_tp, pl.ds(lead + n_ctx, n_lat - lead)])
    load(mod_weight, w_mod)
    load(w_query, weights.at[:, :, pl.ds(0, 128)])
    load(w_key, weights.at[:, :, pl.ds(128, 128)])
    load(w_value, weights.at[:, :, pl.ds(256, 128)])
    load(w_out, w_mix)

    loads[3].wait()
    given = conditions[...]
    activated = (given / (1.0 + jnp.exp(-given))).astype(BF16)
    for j in range(3):
        share = jnp.dot(activated, w_mod[j], preferred_element_type=F32)
        for c in (0, 1) if j < 2 else (0,):
            at = 2 * c + j if j < 2 else 4
            shares[me_sp, :, at * cols : (at + 1) * cols] = share[c : c + 1, :]
    peak[...] = jnp.full(peak.shape, -1e30, F32)
    total[...] = jnp.zeros(total.shape, F32)
    blend[...] = jnp.zeros(blend.shape, F32)
    pl.semaphore_wait(barrier, nsp + ntp - 2)

    def share_copy(k, source):
        return pltpu.make_async_remote_copy(
            shares.at[source],
            shares.at[source],
            share_send.at[k],
            share_recv.at[k],
            device_id={"sp": lax.rem(me_sp + k, nsp)},
            device_id_type=MESH,
        )

    def pair_copy(k, source):
        return pltpu.make_async_remote_copy(
            pairs.at[source],
            pairs.at[source],
            pair_send.at[k],
            pair_recv.at[k],
            device_id={"tp": lax.rem(me_tp + k, ntp)},
            device_id_type=MESH,
        )

    each(1, nsp, lambda k: share_copy(k, me_sp).start())

    def place(c):
        return pl.ds(chunks[c][0], chunks[c][1] + chunks[c][2])

    def rows(c):
        return pl.ds(c * quarter, quarter)

    def tp_block(direction, step, which):
        return lax.rem(chip + nchip + (2 * direction - 1) * step, nchip) * 2 + which

    def z_block(direction, step):
        return lax.rem(me_sp + nsp + (2 * direction - 1) * step, nsp)

    class Ring:
        def __init__(self, buf, at, block, target, send, recv, last):
            self.buf, self.at, self.block, self.target = buf, at, block, target
            self.send, self.recv, self.last = send, recv, last

        def copy(self, direction, step, c, back=1):
            where = self.buf.at[self.block(direction, step - back), self.at(c)]
            return pltpu.make_async_remote_copy(
                where,
                where,
                self.send.at[direction, step - 1, c],
                self.recv.at[direction, step - 1, c],
                device_id=self.target(direction),
                device_id_type=MESH,
            )

        def begin(self, c):
            for d in (0, 1):
                self.copy(d, 1, c).start()

        def advance(self, step, c, after=None):
            for d in (0, 1):
                self.copy(d, step, c, back=0).wait_recv()
                if d == c % 2:
                    self.copy(d, step + 1, c).start()
                else:

                    @pl.when(step < self.last - 1)
                    def _():
                        self.copy(d, step + 1, c).start()

                if after is not None:
                    after(d, step, c)

        def finish(self, c, after=None):
            self.copy(c % 2, self.last, c, back=0).wait_recv()
            if after is not None:
                after(c % 2, self.last, c)

        def sent(self):
            def step_sent(step):
                for c in pieces:
                    for d in (0, 1):
                        self.copy(d, step, c).wait_send()

            each(1, self.last, step_sent)
            for c in pieces:
                self.copy(c % 2, self.last, c).wait_send()

    def tp_target(direction):
        return {"tp": lax.rem(me_tp + (2 if direction == 0 else ntp - 2), ntp)}

    def sp_target(direction):
        return {"sp": lax.rem(me_sp + (1 if direction == 0 else nsp - 1), nsp)}

    def own_block(direction, step):
        return tp_block(direction, step, core)

    x_ring = Ring(feats, place, own_block, tp_target, x_send, x_recv, x_last)
    z_ring = Ring(kv, place, z_block, sp_target, z_send, z_recv, z_last)
    o_ring = Ring(heads, rows, own_block, tp_target, o_send, o_recv, x_last)

    class Mate:
        def __init__(self, buf, at, send, recv):
            self.buf, self.at, self.send, self.recv = buf, at, send, recv

        def copy(self, direction, step, c, which):
            own = isinstance(step, int) and step == 0
            slot = c if own else 4 + ((step - 1) * 2 + direction) * 4 + c
            where = self.buf.at[tp_block(direction, step, which), self.at(c)]
            return pltpu.make_async_remote_copy(
                where,
                where,
                self.send.at[slot],
                self.recv.at[slot],
                device_id={"tp": partner},
                device_id_type=MESH,
            )

        def give(self, direction, step, c):
            self.copy(direction, step, c, core).start()

        def every(self, c, fn):
            fn(0, 0, c)

            def step_fn(step):
                for d in (0, 1):
                    fn(d, step, c)

            each(1, x_last, step_fn)
            fn(c % 2, x_last, c)

    x_mate = Mate(feats, place, d_send, d_recv)
    o_mate = Mate(heads, rows, e_send, e_recv)

    def begin_features(c):
        x_ring.begin(c)
        x_mate.give(0, 0, c)

    loads[0].wait()
    loads[1].wait()
    begin_features(0)
    loads[2].wait()
    begin_features(1)
    begin_features(2)

    def features(step, c):
        x_ring.advance(step, c, x_mate.give)

    def measure(c):
        at, n = chunks[c][0], chunks[c][1] + chunks[c][2]
        x_mate.every(c, lambda d, step, c: x_mate.copy(d, step, c, 1 - core).wait_recv())

        def add_squares(b, carry):
            x = feats[b, at : at + n, :].astype(F32)
            y = x * x
            return carry + y[:, 0:128] + y[:, 128:256]

        squares = lax.fori_loop(0, ntp, add_squares, jnp.zeros((n, 128), F32))
        factor = lax.rsqrt(jnp.sum(squares, axis=1, keepdims=True) * (1.0 / width) + EPS)
        factors[at : at + n, :] = jnp.broadcast_to(factor, (n, 128))

    for c in (0, 1, 2):
        features(1, c)
    for c in (0, 1, 2):
        features(2, c)
    features(3, 0)
    each(1, nsp, lambda k: share_copy(k, lax.rem(me_sp + nsp - k, nsp)).wait_recv())
    modulation = jnp.sum(shares[...], axis=0)
    gate = modulation[:, 4 * cols : 5 * cols]
    gains = gain[...]
    pairs[me_tp, :, 0:cols] = modulation[:, 0:cols]
    pairs[me_tp, :, cols : 2 * cols] = gains * (1.0 + modulation[:, cols : 2 * cols])
    pairs[me_tp, :, 2 * cols : 3 * cols] = modulation[:, 2 * cols : 3 * cols]
    pairs[me_tp, :, 3 * cols : 4 * cols] = gains * (1.0 + modulation[:, 3 * cols : 4 * cols])
    each(1, ntp, lambda k: pair_copy(k, me_tp).start())
    features(3, 1)
    features(3, 2)
    begin_features(3)

    lane = lax.broadcasted_iota(jnp.int32, (1, 2 * DK), 1)
    first_map = lane < DK
    by_row = lax.rem(lane, DK) < DK // 2
    lower = lax.rem(lane, DK // 2) < DK // 4
    grid_rows = n_lat // GRID_W
    table_rows = nsp * grid_rows

    def head_norm(x, g):
        squared = x * x
        one = jnp.sum(jnp.where(first_map, squared, 0.0), axis=1, keepdims=True)
        two = jnp.sum(jnp.where(first_map, 0.0, squared), axis=1, keepdims=True)
        scale = jnp.where(
            first_map, lax.rsqrt(one * (1.0 / DK) + EPS), lax.rsqrt(two * (1.0 / DK) + EPS)
        )
        return x * scale * g

    def positions(table, first, n):
        mine = table[pl.ds(pl.multiple_of(me_sp * grid_rows, grid_rows), grid_rows), :]
        columns = table[table_rows : table_rows + GRID_W, :]
        return jnp.concatenate(
            [
                jnp.where(by_row, mine[g : g + 1, :], columns)
                for g in range(first // GRID_W, (first + n) // GRID_W)
            ],
            axis=0,
        )

    def turn(x, cosine, sine):
        other = jnp.where(
            lower, pltpu.roll(x, 2 * DK - DK // 4, axis=1), pltpu.roll(x, DK // 4, axis=1)
        )
        return x * cosine + other * sine

    q_gain = jnp.concatenate([query_gain[...], query_gain[...]], axis=1) * (DK**-0.5 * LOG2E)
    k_gain = jnp.concatenate([key_gain[...], key_gain[...]], axis=1)

    def project(c):
        at, n_here, n_more, first = chunks[c]
        n = n_here + n_more
        proj[0:n, :] = jnp.zeros((n, 3 * DV), F32)

        def modulated(b, start, count, column):
            x = feats[b, at + start : at + start + count, :].astype(F32)
            f = factors[at + start : at + start + count, :]
            f = jnp.concatenate([f, f], axis=1)
            shift = pairs[b, :, column * cols : (column + 1) * cols]
            scale = pairs[b, :, (column + 1) * cols : (column + 2) * cols]
            return (x * f * scale + shift).astype(BF16)

        def add_block(b, carry):
            x = modulated(b, 0, n_here, 0)
            if n_more:
                x = jnp.concatenate([x, modulated(b, n_here, n_more, 2)], axis=0)
            proj[0:n, :] += jnp.dot(x, weights[b], preferred_element_type=F32)
            return carry

        lax.fori_loop(0, ntp, add_block, 0, unroll=4)
        cosine, sine = positions(cos_table, first, n_here), positions(sin_table, first, n_here)
        k = turn(head_norm(proj[0:n_here, 128:256], k_gain), cosine, sine)
        kv[me_sp, at : at + n_here, 0:128] = k.astype(BF16)
        if n_more:
            kv[me_sp, at + n_here : at + n, 0:128] = head_norm(
                proj[n_here:n, 128:256], k_gain
            ).astype(BF16)
        kv[me_sp, at : at + n, 128:256] = proj[0:n, 256:384].astype(BF16)
        q = turn(head_norm(proj[0:n_here, 0:128], q_gain), cosine, sine)
        queries[0, first : first + n_here, :] = jnp.where(first_map, q, 0.0).astype(BF16)
        queries[1, first : first + n_here, :] = jnp.where(first_map, 0.0, q).astype(BF16)
        z_ring.begin(c)

    def piece(block, c, lanes):
        at, n = chunks[c][0], chunks[c][1] + chunks[c][2]
        return kv[block, at : at + n, lanes[0] : lanes[1]]

    def absorb_half(parts, h):
        for m in (0, 1):
            i = 2 * m + h
            q = queries[m, h * half : (h + 1) * half, :]
            scores = [
                lax.dot_general(
                    piece(block, c, (0, 2 * DK)),
                    q,
                    (((1,), (1,)), ((), ())),
                    preferred_element_type=F32,
                )
                for block, c in parts
            ]
            old = peak[i]
            new = old
            for s in scores:
                new = jnp.maximum(new, jnp.max(s, axis=0, keepdims=True))
            rescale = jnp.exp2(old - new)
            summed, mixture = total[i] * rescale, blend[i] * rescale
            for (block, c), s in zip(parts, scores):
                expo = jnp.exp2(s - new)
                summed += jnp.sum(expo, axis=0, keepdims=True)
                mixture += lax.dot_general(
                    piece(block, c, (2 * DK, 2 * DK + DV)),
                    expo.astype(BF16),
                    (((0,), (0,)), ((), ())),
                    preferred_element_type=F32,
                )
            total[i], blend[i], peak[i] = summed, mixture, new

    def absorb(parts):
        for h in (0, 1):
            absorb_half(parts, h)

    def take(step, c):
        absorb([(z_block(0, step), c), (z_block(1, step), c)])

    move = z_ring.advance
    x_ring.finish(0, x_mate.give)
    x_ring.finish(1, x_mate.give)
    measure(0)
    for one in loads[4:7]:
        one.wait()
    each(1, ntp, lambda k: pair_copy(k, lax.rem(me_tp + ntp - k, ntp)).wait_recv())
    project(0)
    x_ring.finish(2, x_mate.give)
    measure(1)
    features(1, 3)
    project(1)
    measure(2)
    project(2)
    move(1, 0)
    features(2, 3)
    move(1, 1)
    move(1, 2)
    move(2, 0)
    features(3, 3)
    move(2, 1)
    move(2, 2)
    x_ring.finish(3, x_mate.give)
    measure(3)
    project(3)
    move(3, 0)
    move(3, 1)
    absorb([(me_sp, 0), (me_sp, 1)])
    move(3, 2)
    absorb([(me_sp, 2), (me_sp, 3)])
    move(1, 3)
    take(1, 0)
    take(1, 1)
    take(1, 2)

    def mingled(j):
        a, b = 4 + 2 * j, 2 + 3 * j
        move(a, 0)
        take(a - 2, 0)
        move(a, 1)
        take(a - 2, 1)
        move(b, 3)
        take(b - 1, 3)
        move(a, 2)
        take(a - 2, 2)
        move(a + 1, 0)
        take(a - 1, 0)
        move(b + 1, 3)
        take(b, 3)
        move(a + 1, 1)
        take(a - 1, 1)
        move(a + 1, 2)
        take(a - 1, 2)
        move(b + 2, 3)
        take(b + 1, 3)

    rounds = z_last // 2 - 2
    each(0, rounds, mingled)
    early, late = 4 + 2 * rounds, 2 + 3 * rounds
    for step in range(early, z_last):
        for c in (0, 1, 2):
            move(step, c)
            take(step - 2, c)
    for step in range(late, z_last):
        move(step, 3)
        take(step - 1, 3)
    for c in (0, 1, 2):
        take(z_last - 2, c)
        z_ring.finish(c)
        take(z_last - 1, c)
    take(z_last - 1, 3)
    absorb([(z_block(0, z_last), 0), (z_block(1, z_last), 1)])
    z_ring.finish(3)

    loads[7].wait()
    weight = lambdas[0]
    for h in (0, 1):
        absorb_half([(z_block(0, z_last), 2), (z_block(1, z_last), 3)], h)
        attended = blend[h] * (1.0 / total[h]) - blend[2 + h] * (weight / total[2 + h])
        scale = lax.rsqrt(jnp.sum(attended * attended, axis=0, keepdims=True) * (1.0 / DV) + EPS)
        heads[me_tp, h * half : (h + 1) * half, :] = (
            jnp.transpose(attended * scale) * out_gain[...]
        ).astype(BF16)
        for c in (2 * h, 2 * h + 1):
            o_ring.begin(c)
            o_mate.give(0, 0, c)

    def mix(direction, step, c):
        o_mate.copy(direction, step, c, 1 - core).wait_recv()
        first = tp_block(direction, step, 0)
        at = c * quarter
        both = jnp.concatenate(
            [heads[first, at : at + quarter, :], heads[first + 1, at : at + quarter, :]], axis=1
        )
        piece = jnp.dot(both, w_mix[lax.div(first, 2)], preferred_element_type=F32)
        if isinstance(step, int) and step == 0:
            mixed[at : at + quarter, :] = piece
        else:
            mixed[at : at + quarter, :] += piece

    def mix_all(step):
        for c in pieces:
            for d in (0, 1):
                mix(d, step, c)

    def out_step(step):
        for c in pieces:
            o_ring.advance(step, c, o_mate.give)
        mix_all(step - 1)

    for c in pieces:
        o_ring.advance(1, c, o_mate.give)
    for c in pieces:
        mix(0, 0, c)
    each(2, x_last, out_step)
    for c in pieces:
        o_ring.finish(c, o_mate.give)
    mix_all(x_last - 1)
    for c in pieces:
        mix(c % 2, x_last, c)
        at = c * quarter
        for start, count in ((at, lead), (at + lead, quarter - lead)):
            shift = 0 if start < lead else n_ctx
            mine = feats[me_tp, start + shift : start + shift + count, :].astype(F32)
            out[start : start + count, :] = (
                mine + gate * mixed[start : start + count, :]
            ).astype(BF16)

    each(1, nsp, lambda k: share_copy(k, me_sp).wait_send())
    each(1, ntp, lambda k: pair_copy(k, me_tp).wait_send())
    for ring in (x_ring, z_ring, o_ring):
        ring.sent()
    for mate in (x_mate, o_mate):
        for c in pieces:
            mate.every(c, lambda d, step, c: mate.copy(d, step, c, core).wait_send())


def local(
    latent,
    context,
    conditions,
    mod_weight,
    norm_gain,
    w_query,
    w_key,
    w_value,
    query_gain,
    key_gain,
    lambdas,
    out_gain,
    w_out,
):
    nsp, ntp = lax.axis_size("sp"), lax.axis_size("tp")
    n_lat, cols = latent.shape
    n_ctx = context.shape[0]
    block = n_lat + n_ctx
    half = n_lat // 2
    nchip = ntp // 2
    n_in = mod_weight.shape[0]
    cosine, sine = angle_tables(nsp * n_lat // GRID_W)
    vmem = pl.BlockSpec(memory_space=pltpu.VMEM)
    smem = pl.BlockSpec(memory_space=pltpu.SMEM)
    hbm = pl.BlockSpec(memory_space=pl.ANY)
    dma = pltpu.SemaphoreType.DMA
    return pl.pallas_call(
        functools.partial(kernel, nsp, ntp),
        out_shape=jax.ShapeDtypeStruct((n_lat, cols), BF16),
        in_specs=[hbm, hbm, vmem, hbm, vmem]
        + [hbm, hbm, hbm, vmem, vmem, smem, vmem, hbm, vmem, vmem],
        out_specs=vmem,
        scratch_shapes=[
            pltpu.VMEM((ntp, block, cols), BF16),
            pltpu.VMEM((3, n_in, cols), BF16),
            pltpu.VMEM((ntp, cols, 3 * DV), BF16),
            pltpu.VMEM((nchip, 2 * DV, cols), BF16),
            pltpu.VMEM((nsp, 1, 5 * cols), F32),
            pltpu.VMEM((ntp, 1, 4 * cols), F32),
            pltpu.VMEM((block, 128), F32),
            pltpu.VMEM((block, 3 * DV), F32),
            pltpu.VMEM((2, n_lat, 2 * DK), BF16),
            pltpu.VMEM((nsp, block, 2 * DK + DV), BF16),
            pltpu.VMEM((4, 1, half), F32),
            pltpu.VMEM((4, 1, half), F32),
            pltpu.VMEM((4, DV, half), F32),
            pltpu.VMEM((ntp, n_lat, DV), BF16),
            pltpu.VMEM((n_lat, cols), F32),
            dma((8,)),
            dma((nsp,)),
            dma((nsp,)),
            dma((ntp,)),
            dma((ntp,)),
            dma((2, nchip // 2, 4)),
            dma((2, nchip // 2, 4)),
            dma((4 + 4 * nchip,)),
            dma((4 + 4 * nchip,)),
            dma((2, nsp // 2, 4)),
            dma((2, nsp // 2, 4)),
            dma((2, nchip // 2, 4)),
            dma((2, nchip // 2, 4)),
            dma((4 + 4 * nchip,)),
            dma((4 + 4 * nchip,)),
        ],
        compiler_params=pltpu.CompilerParams(collective_id=0, has_side_effects=True),
    )(
        latent,
        context,
        conditions,
        jnp.transpose(mod_weight, (1, 0, 2)),
        norm_gain[None],
        w_query.reshape(ntp, cols, DV),
        w_key.reshape(ntp, cols, DV),
        w_value.reshape(ntp, cols, DV),
        query_gain[None],
        key_gain[None],
        lambdas,
        out_gain[None],
        w_out.reshape(nchip, 2 * DV, cols),
        jnp.asarray(cosine),
        jnp.asarray(sine),
    )


def solution(mesh):
    in_specs = (
        P(("grp", "sp"), "tp"),
        P(("grp", "sp"), "tp"),
        P("grp", "sp"),
        P("sp", None, "tp"),
        P("tp"),
        P(None, "tp"),
        P(None, "tp"),
        P(None, "tp"),
        P(),
        P(),
        P("tp"),
        P(),
        P(None, "tp"),
    )
    out_specs = P(("grp", "sp"), "tp")
    return jax.shard_map(local, mesh=mesh, in_specs=in_specs, out_specs=out_specs, check_vma=False)
```

```python
import functools

import jax
import jax.numpy as jnp
import numpy as np
from jax import lax
from jax.experimental import pallas as pl
from jax.experimental.pallas import tpu as pltpu
from jax.sharding import PartitionSpec as P

DK = 64
DV = 128
GRID_W = 64
EPS = 1e-06
LOG2E = 1.4426950408889634
MESH = pl.DeviceIdType.MESH
F32 = jnp.float32
BF16 = jnp.bfloat16


def angle_tables(grid_rows):
    half, quarter = DK // 2, DK // 4
    lane = np.arange(2 * DK) % DK
    inverse = (10000.0 ** (-2.0 * (lane % quarter) / half)).astype(np.float32)
    sign = np.where(lane % half < quarter, -1.0, 1.0).astype(np.float32)
    places = np.concatenate([np.arange(grid_rows), np.arange(GRID_W)]).astype(np.float32)
    angles = (places[:, None] * inverse[None, :]).astype(np.float32).astype(np.float64)
    return np.cos(angles).astype(np.float32), (np.sin(angles) * sign).astype(np.float32)


def kernel(
    nsp,
    ntp,
    latent,
    context,
    conditions,
    mod_weight,
    gain,
    w_query,
    w_key,
    w_value,
    query_gain,
    key_gain,
    lambdas,
    out_gain,
    w_out,
    cos_table,
    sin_table,
    out,
    feats,
    w_mod,
    weights,
    w_mix,
    shares,
    pairs,
    factors,
    proj,
    queries,
    kv,
    peak,
    total,
    blend,
    heads,
    mixed,
    load_sem,
    share_send,
    share_recv,
    pair_send,
    pair_recv,
    x_send,
    x_recv,
    d_send,
    d_recv,
    z_send,
    z_recv,
    o_send,
    o_recv,
    e_send,
    e_recv,
):
    me_sp, me_tp = lax.axis_index("sp"), lax.axis_index("tp")
    core, chip = lax.rem(me_tp, 2), lax.div(me_tp, 2)
    nchip = ntp // 2
    x_last, z_last = nchip // 2, nsp // 2
    partner = me_tp + 1 - 2 * core
    n_lat, cols = latent.shape
    n_ctx = context.shape[0]
    half, quarter = n_lat // 2, n_lat // 4
    width = cols * ntp
    lead = GRID_W
    chunks = (
        (0, lead, n_ctx, 0),
        (lead + n_ctx, quarter, 0, lead),
        (lead + n_ctx + quarter, quarter, 0, lead + quarter),
        (lead + n_ctx + 2 * quarter, quarter, 0, lead + 2 * quarter),
        (lead + n_ctx + 3 * quarter, lead, 0, lead + 3 * quarter),
    )
    pieces = range(4)

    barrier = pltpu.get_barrier_semaphore()

    def each(first, last, fn):
        def step(k, carry):
            fn(k)
            return carry

        lax.fori_loop(first, last, step, 0)

    def greet(axis, target):
        pl.semaphore_signal(barrier, 1, device_id={axis: target}, device_id_type=MESH)

    each(1, ntp, lambda k: greet("tp", lax.rem(me_tp + k, ntp)))
    each(1, nsp, lambda k: greet("sp", lax.rem(me_sp + k, nsp)))

    loads = []

    def load(src, dst):
        loads.append(pltpu.make_async_copy(src, dst, load_sem.at[len(loads)]))
        loads[-1].start()

    load(latent.at[pl.ds(0, lead)], feats.at[me_tp, pl.ds(0, lead)])
    load(context, feats.at[me_tp, pl.ds(lead, n_ctx)])
    load(latent.at[pl.ds(lead, n_lat - lead)], feats.at[me_tp, pl.ds(lead + n_ctx, n_lat - lead)])
    load(mod_weight, w_mod)
    load(w_query, weights.at[:, :, pl.ds(0, 128)])
    load(w_key, weights.at[:, :, pl.ds(128, 128)])
    load(w_value, weights.at[:, :, pl.ds(256, 128)])
    load(w_out, w_mix)

    loads[3].wait()
    given = conditions[...]
    activated = (given / (1.0 + jnp.exp(-given))).astype(BF16)
    for j in range(3):
        share = jnp.dot(activated, w_mod[j], preferred_element_type=F32)
        for c in (0, 1) if j < 2 else (0,):
            at = 2 * c + j if j < 2 else 4
            shares[me_sp, :, at * cols : (at + 1) * cols] = share[c : c + 1, :]
    peak[...] = jnp.full(peak.shape, -1e30, F32)
    total[...] = jnp.zeros(total.shape, F32)
    blend[...] = jnp.zeros(blend.shape, F32)
    pl.semaphore_wait(barrier, nsp + ntp - 2)

    def share_copy(k, source):
        return pltpu.make_async_remote_copy(
            shares.at[source],
            shares.at[source],
            share_send.at[k],
            share_recv.at[k],
            device_id={"sp": lax.rem(me_sp + k, nsp)},
            device_id_type=MESH,
        )

    def pair_copy(k, source):
        return pltpu.make_async_remote_copy(
            pairs.at[source],
            pairs.at[source],
            pair_send.at[k],
            pair_recv.at[k],
            device_id={"tp": lax.rem(me_tp + k, ntp)},
            device_id_type=MESH,
        )

    each(1, nsp, lambda k: share_copy(k, me_sp).start())

    def place(c):
        return pl.ds(chunks[c][0], chunks[c][1] + chunks[c][2])

    def rows(c):
        return pl.ds(c * quarter, quarter)

    def tp_block(direction, step, which):
        return lax.rem(chip + nchip + (2 * direction - 1) * step, nchip) * 2 + which

    def z_block(direction, step):
        return lax.rem(me_sp + nsp + (2 * direction - 1) * step, nsp)

    class Ring:
        def __init__(self, buf, at, block, target, send, recv, last, pieces):
            self.buf, self.at, self.block, self.target = buf, at, block, target
            self.send, self.recv, self.last, self.pieces = send, recv, last, pieces

        def copy(self, direction, step, c, back=1):
            where = self.buf.at[self.block(direction, step - back), self.at(c)]
            return pltpu.make_async_remote_copy(
                where,
                where,
                self.send.at[direction, step - 1, c],
                self.recv.at[direction, step - 1, c],
                device_id=self.target(direction),
                device_id_type=MESH,
            )

        def begin(self, c):
            for d in (0, 1):
                self.copy(d, 1, c).start()

        def advance(self, step, c, after=None):
            for d in (0, 1):
                self.copy(d, step, c, back=0).wait_recv()
                if d == c % 2:
                    self.copy(d, step + 1, c).start()
                else:

                    @pl.when(step < self.last - 1)
                    def _():
                        self.copy(d, step + 1, c).start()

                if after is not None:
                    after(d, step, c)

        def finish(self, c, after=None):
            self.copy(c % 2, self.last, c, back=0).wait_recv()
            if after is not None:
                after(c % 2, self.last, c)

        def sent(self):
            def step_sent(step):
                for c in self.pieces:
                    for d in (0, 1):
                        self.copy(d, step, c).wait_send()

            each(1, self.last, step_sent)
            for c in self.pieces:
                self.copy(c % 2, self.last, c).wait_send()

    def tp_target(direction):
        return {"tp": lax.rem(me_tp + (2 if direction == 0 else ntp - 2), ntp)}

    def sp_target(direction):
        return {"sp": lax.rem(me_sp + (1 if direction == 0 else nsp - 1), nsp)}

    def own_block(direction, step):
        return tp_block(direction, step, core)

    x_ring = Ring(feats, place, own_block, tp_target, x_send, x_recv, x_last, range(5))
    z_ring = Ring(kv, place, z_block, sp_target, z_send, z_recv, z_last, range(5))
    o_ring = Ring(heads, rows, own_block, tp_target, o_send, o_recv, x_last, pieces)

    class Mate:
        def __init__(self, buf, at, send, recv, pieces):
            self.buf, self.at, self.send, self.recv = buf, at, send, recv
            self.pieces = pieces

        def copy(self, direction, step, c, which):
            own = isinstance(step, int) and step == 0
            count = len(self.pieces)
            slot = c if own else count + ((step - 1) * 2 + direction) * count + c
            where = self.buf.at[tp_block(direction, step, which), self.at(c)]
            return pltpu.make_async_remote_copy(
                where,
                where,
                self.send.at[slot],
                self.recv.at[slot],
                device_id={"tp": partner},
                device_id_type=MESH,
            )

        def give(self, direction, step, c):
            self.copy(direction, step, c, core).start()

        def every(self, c, fn):
            fn(0, 0, c)

            def step_fn(step):
                for d in (0, 1):
                    fn(d, step, c)

            each(1, x_last, step_fn)
            fn(c % 2, x_last, c)

    x_mate = Mate(feats, place, d_send, d_recv, range(5))
    o_mate = Mate(heads, rows, e_send, e_recv, pieces)

    def begin_features(c):
        x_ring.begin(c)
        x_mate.give(0, 0, c)

    loads[0].wait()
    loads[1].wait()
    begin_features(0)
    loads[2].wait()
    begin_features(1)
    begin_features(2)

    def features(step, c):
        x_ring.advance(step, c, x_mate.give)

    def measure(c):
        at, n = chunks[c][0], chunks[c][1] + chunks[c][2]
        x_mate.every(c, lambda d, step, c: x_mate.copy(d, step, c, 1 - core).wait_recv())

        def add_squares(b, carry):
            x = feats[b, at : at + n, :].astype(F32)
            y = x * x
            return carry + y[:, 0:128] + y[:, 128:256]

        squares = lax.fori_loop(0, ntp, add_squares, jnp.zeros((n, 128), F32))
        factor = lax.rsqrt(jnp.sum(squares, axis=1, keepdims=True) * (1.0 / width) + EPS)
        factors[at : at + n, :] = jnp.broadcast_to(factor, (n, 128))

    for c in (0, 1, 2):
        features(1, c)
    for c in (0, 1, 2):
        features(2, c)
    features(3, 0)
    each(1, nsp, lambda k: share_copy(k, lax.rem(me_sp + nsp - k, nsp)).wait_recv())
    modulation = jnp.sum(shares[...], axis=0)
    gate = modulation[:, 4 * cols : 5 * cols]
    gains = gain[...]
    pairs[me_tp, :, 0:cols] = modulation[:, 0:cols]
    pairs[me_tp, :, cols : 2 * cols] = gains * (1.0 + modulation[:, cols : 2 * cols])
    pairs[me_tp, :, 2 * cols : 3 * cols] = modulation[:, 2 * cols : 3 * cols]
    pairs[me_tp, :, 3 * cols : 4 * cols] = gains * (1.0 + modulation[:, 3 * cols : 4 * cols])
    each(1, ntp, lambda k: pair_copy(k, me_tp).start())
    features(3, 1)
    features(3, 2)
    begin_features(3)
    begin_features(4)

    lane = lax.broadcasted_iota(jnp.int32, (1, 2 * DK), 1)
    first_map = lane < DK
    by_row = lax.rem(lane, DK) < DK // 2
    lower = lax.rem(lane, DK // 2) < DK // 4
    grid_rows = n_lat // GRID_W
    table_rows = nsp * grid_rows

    def head_norm(x, g):
        squared = x * x
        one = jnp.sum(jnp.where(first_map, squared, 0.0), axis=1, keepdims=True)
        two = jnp.sum(jnp.where(first_map, 0.0, squared), axis=1, keepdims=True)
        scale = jnp.where(
            first_map, lax.rsqrt(one * (1.0 / DK) + EPS), lax.rsqrt(two * (1.0 / DK) + EPS)
        )
        return x * scale * g

    def positions(table, first, n):
        mine = table[pl.ds(pl.multiple_of(me_sp * grid_rows, grid_rows), grid_rows), :]
        columns = table[table_rows : table_rows + GRID_W, :]
        return jnp.concatenate(
            [
                jnp.where(by_row, mine[g : g + 1, :], columns)
                for g in range(first // GRID_W, (first + n) // GRID_W)
            ],
            axis=0,
        )

    def turn(x, cosine, sine):
        other = jnp.where(
            lower, pltpu.roll(x, 2 * DK - DK // 4, axis=1), pltpu.roll(x, DK // 4, axis=1)
        )
        return x * cosine + other * sine

    q_gain = jnp.concatenate([query_gain[...], query_gain[...]], axis=1) * (DK**-0.5 * LOG2E)
    k_gain = jnp.concatenate([key_gain[...], key_gain[...]], axis=1)

    def project(c):
        at, n_here, n_more, first = chunks[c]
        n = n_here + n_more
        proj[0:n, :] = jnp.zeros((n, 3 * DV), F32)

        def modulated(b, start, count, column):
            x = feats[b, at + start : at + start + count, :].astype(F32)
            f = factors[at + start : at + start + count, :]
            f = jnp.concatenate([f, f], axis=1)
            shift = pairs[b, :, column * cols : (column + 1) * cols]
            scale = pairs[b, :, (column + 1) * cols : (column + 2) * cols]
            return (x * f * scale + shift).astype(BF16)

        group = 4

        def add_blocks(g, carry):
            inputs = []
            for b in range(group):
                x = modulated(g * group + b, 0, n_here, 0)
                if n_more:
                    x = jnp.concatenate([x, modulated(g * group + b, n_here, n_more, 2)], axis=0)
                inputs.append(x)
            matrix = weights[pl.ds(g * group, group)].reshape(group * cols, 3 * DV)
            proj[0:n, :] += jnp.dot(
                jnp.concatenate(inputs, axis=1), matrix, preferred_element_type=F32
            )
            return carry

        lax.fori_loop(0, ntp // group, add_blocks, 0)
        cosine, sine = positions(cos_table, first, n_here), positions(sin_table, first, n_here)
        k = turn(head_norm(proj[0:n_here, 128:256], k_gain), cosine, sine)
        kv[me_sp, at : at + n_here, 0:128] = k.astype(BF16)
        if n_more:
            kv[me_sp, at + n_here : at + n, 0:128] = head_norm(
                proj[n_here:n, 128:256], k_gain
            ).astype(BF16)
        kv[me_sp, at : at + n, 128:256] = proj[0:n, 256:384].astype(BF16)
        q = turn(head_norm(proj[0:n_here, 0:128], q_gain), cosine, sine)
        queries[0, first : first + n_here, :] = jnp.where(first_map, q, 0.0).astype(BF16)
        queries[1, first : first + n_here, :] = jnp.where(first_map, 0.0, q).astype(BF16)
        z_ring.begin(c)

    def piece(block, c, lanes):
        at, n = chunks[c][0], chunks[c][1] + chunks[c][2]
        return kv[block, at : at + n, lanes[0] : lanes[1]]

    def absorb_half(parts, h):
        for m in (0, 1):
            i = 2 * m + h
            q = queries[m, h * half : (h + 1) * half, :]
            scores = [
                lax.dot_general(
                    piece(block, c, (0, 2 * DK)),
                    q,
                    (((1,), (1,)), ((), ())),
                    preferred_element_type=F32,
                )
                for block, c in parts
            ]
            old = peak[i]
            new = old
            for s in scores:
                new = jnp.maximum(new, jnp.max(s, axis=0, keepdims=True))
            rescale = jnp.exp2(old - new)
            summed, mixture = total[i] * rescale, blend[i] * rescale
            for (block, c), s in zip(parts, scores):
                expo = jnp.exp2(s - new)
                summed += jnp.sum(expo, axis=0, keepdims=True)
                mixture += lax.dot_general(
                    piece(block, c, (2 * DK, 2 * DK + DV)),
                    expo.astype(BF16),
                    (((0,), (0,)), ((), ())),
                    preferred_element_type=F32,
                )
            total[i], blend[i], peak[i] = summed, mixture, new

    def absorb(parts):
        for h in (0, 1):
            absorb_half(parts, h)

    def take(step, c):
        absorb([(z_block(0, step), c), (z_block(1, step), c)])

    move = z_ring.advance
    x_ring.finish(0, x_mate.give)
    x_ring.finish(1, x_mate.give)
    measure(0)
    for one in loads[4:7]:
        one.wait()
    each(1, ntp, lambda k: pair_copy(k, lax.rem(me_tp + ntp - k, ntp)).wait_recv())
    project(0)
    x_ring.finish(2, x_mate.give)
    measure(1)
    features(1, 3)
    features(1, 4)
    project(1)
    measure(2)
    project(2)
    move(1, 0)
    features(2, 3)
    features(2, 4)
    move(1, 1)
    move(1, 2)
    features(3, 3)
    move(2, 0)
    features(3, 4)
    move(2, 1)
    x_ring.finish(3, x_mate.give)
    move(2, 2)
    measure(3)
    project(3)
    x_ring.finish(4, x_mate.give)
    move(3, 0)
    measure(4)
    project(4)
    move(3, 1)
    absorb([(me_sp, 0), (me_sp, 1)])
    move(3, 2)
    absorb([(me_sp, 2), (me_sp, 3), (me_sp, 4)])
    others = [(step, c) for step in range(4, z_last + 1) for c in (0, 1, 2)]
    lasts = [(step, c) for step in range(1, z_last) for c in (3, 4)]
    order = []
    while others or lasts:
        order += others[:1] + lasts[:1]
        others, lasts = others[1:], lasts[1:]
    waiting = [(step, c) for step in (1, 2, 3) for c in (0, 1, 2)]

    def take_some(count):
        for _ in range(min(count, len(waiting))):
            take(*waiting.pop(0))

    take_some(3)
    for step, c in order:
        if step < z_last:
            move(step, c)
            waiting.append((step, c))
        else:
            z_ring.finish(c)
        take_some(2 if len(waiting) > 5 else 1)
    take_some(len(waiting))
    absorb([(z_block(0, z_last), 0), (z_block(1, z_last), 1)])
    z_ring.finish(3)
    z_ring.finish(4)

    loads[7].wait()
    weight = lambdas[0]
    for h in (0, 1):
        absorb_half([(z_block(0, z_last), 2), (z_block(1, z_last), 3), (z_block(0, z_last), 4)], h)
        attended = blend[h] * (1.0 / total[h]) - blend[2 + h] * (weight / total[2 + h])
        scale = lax.rsqrt(jnp.sum(attended * attended, axis=0, keepdims=True) * (1.0 / DV) + EPS)
        heads[me_tp, h * half : (h + 1) * half, :] = (
            jnp.transpose(attended * scale) * out_gain[...]
        ).astype(BF16)
        for c in (2 * h, 2 * h + 1):
            o_ring.begin(c)
            o_mate.give(0, 0, c)

    def mix(direction, step, c):
        o_mate.copy(direction, step, c, 1 - core).wait_recv()
        first = tp_block(direction, step, 0)
        at = c * quarter
        both = jnp.concatenate(
            [heads[first, at : at + quarter, :], heads[first + 1, at : at + quarter, :]], axis=1
        )
        piece = jnp.dot(both, w_mix[lax.div(first, 2)], preferred_element_type=F32)
        if isinstance(step, int) and step == 0:
            mixed[at : at + quarter, :] = piece
        else:
            mixed[at : at + quarter, :] += piece

    def mix_both(step, c):
        for d in (0, 1):
            mix(d, step, c)

    for c in pieces:
        o_ring.advance(1, c, o_mate.give)
        mix(0, 0, c)

    def out_step(step):
        for c in pieces:
            o_ring.advance(step, c, o_mate.give)
            mix_both(step - 1, c)

    each(2, x_last, out_step)
    for c in pieces:
        o_ring.finish(c, o_mate.give)
        mix_both(x_last - 1, c)
    for c in pieces:
        mix(c % 2, x_last, c)
        at = c * quarter
        for start, count in ((at, lead), (at + lead, quarter - lead)):
            shift = 0 if start < lead else n_ctx
            mine = feats[me_tp, start + shift : start + shift + count, :].astype(F32)
            out[start : start + count, :] = (
                mine + gate * mixed[start : start + count, :]
            ).astype(BF16)

    each(1, nsp, lambda k: share_copy(k, me_sp).wait_send())
    each(1, ntp, lambda k: pair_copy(k, me_tp).wait_send())
    for ring in (x_ring, z_ring, o_ring):
        ring.sent()
    for mate in (x_mate, o_mate):
        for c in mate.pieces:
            mate.every(c, lambda d, step, c: mate.copy(d, step, c, core).wait_send())


def local(
    latent,
    context,
    conditions,
    mod_weight,
    norm_gain,
    w_query,
    w_key,
    w_value,
    query_gain,
    key_gain,
    lambdas,
    out_gain,
    w_out,
):
    nsp, ntp = lax.axis_size("sp"), lax.axis_size("tp")
    n_lat, cols = latent.shape
    n_ctx = context.shape[0]
    block = n_lat + n_ctx
    half = n_lat // 2
    nchip = ntp // 2
    n_in = mod_weight.shape[0]
    cosine, sine = angle_tables(nsp * n_lat // GRID_W)
    vmem = pl.BlockSpec(memory_space=pltpu.VMEM)
    smem = pl.BlockSpec(memory_space=pltpu.SMEM)
    hbm = pl.BlockSpec(memory_space=pl.ANY)
    dma = pltpu.SemaphoreType.DMA
    return pl.pallas_call(
        functools.partial(kernel, nsp, ntp),
        out_shape=jax.ShapeDtypeStruct((n_lat, cols), BF16),
        in_specs=[hbm, hbm, vmem, hbm, vmem]
        + [hbm, hbm, hbm, vmem, vmem, smem, vmem, hbm, vmem, vmem],
        out_specs=vmem,
        scratch_shapes=[
            pltpu.VMEM((ntp, block, cols), BF16),
            pltpu.VMEM((3, n_in, cols), BF16),
            pltpu.VMEM((ntp, cols, 3 * DV), BF16),
            pltpu.VMEM((nchip, 2 * DV, cols), BF16),
            pltpu.VMEM((nsp, 1, 5 * cols), F32),
            pltpu.VMEM((ntp, 1, 4 * cols), F32),
            pltpu.VMEM((block, 128), F32),
            pltpu.VMEM((block, 3 * DV), F32),
            pltpu.VMEM((2, n_lat, 2 * DK), BF16),
            pltpu.VMEM((nsp, block, 2 * DK + DV), BF16),
            pltpu.VMEM((4, 1, half), F32),
            pltpu.VMEM((4, 1, half), F32),
            pltpu.VMEM((4, DV, half), F32),
            pltpu.VMEM((ntp, n_lat, DV), BF16),
            pltpu.VMEM((n_lat, cols), F32),
            dma((8,)),
            dma((nsp,)),
            dma((nsp,)),
            dma((ntp,)),
            dma((ntp,)),
            dma((2, nchip // 2, 5)),
            dma((2, nchip // 2, 5)),
            dma((5 + 5 * nchip,)),
            dma((5 + 5 * nchip,)),
            dma((2, nsp // 2, 5)),
            dma((2, nsp // 2, 5)),
            dma((2, nchip // 2, 4)),
            dma((2, nchip // 2, 4)),
            dma((4 + 4 * nchip,)),
            dma((4 + 4 * nchip,)),
        ],
        compiler_params=pltpu.CompilerParams(collective_id=0, has_side_effects=True),
    )(
        latent,
        context,
        conditions,
        jnp.transpose(mod_weight, (1, 0, 2)),
        norm_gain[None],
        w_query.reshape(ntp, cols, DV),
        w_key.reshape(ntp, cols, DV),
        w_value.reshape(ntp, cols, DV),
        query_gain[None],
        key_gain[None],
        lambdas,
        out_gain[None],
        w_out.reshape(nchip, 2 * DV, cols),
        jnp.asarray(cosine),
        jnp.asarray(sine),
    )


def solution(mesh):
    in_specs = (
        P(("grp", "sp"), "tp"),
        P(("grp", "sp"), "tp"),
        P("grp", "sp"),
        P("sp", None, "tp"),
        P("tp"),
        P(None, "tp"),
        P(None, "tp"),
        P(None, "tp"),
        P(),
        P(),
        P("tp"),
        P(),
        P(None, "tp"),
    )
    out_specs = P(("grp", "sp"), "tp")
    return jax.shard_map(local, mesh=mesh, in_specs=in_specs, out_specs=out_specs, check_vma=False)
```
